256 devices in a mesh: ep: 128 (over z, y, x), tp: 2 (over core).
Axes of the slice: x: 4, y: 4, z: 8, core: 2. Of those that a mesh axis runs over, the one named last changes fastest.
Arguments:
- tokens: bfloat16 [16384, 2048], P('ep', 'tp'), may hold values from -24 to 24
- cotangent: bfloat16 [16384, 2048], P('ep', 'tp'), may hold values from -24 to 24
- routes: int32 [16384, 2], P('ep'), may hold values from 0 to 127, all different within a row; in each aligned block of 128 rows (0 to 127, 128 to 255, ...) at most 3 rows name the same one
- route_weights: float32 [16384, 2], P('ep'), may hold values from 0.1 to 2.5
- gate_proj: bfloat16 [128, 2048, 512], P('ep', None, 'tp'), may hold values from -0.125 to 0.125
- up_proj: bfloat16 [128, 2048, 512], P('ep', None, 'tp'), may hold values from -0.125 to 0.125
- down_proj: bfloat16 [128, 512, 2048], P('ep', 'tp'), may hold values from -0.25 to 0.25
- shared_gate: bfloat16 [2048, 512], P(None, 'tp'), may hold values from -0.125 to 0.125
- shared_up: bfloat16 [2048, 512], P(None, 'tp'), may hold values from -0.125 to 0.125
- shared_down: bfloat16 [2048, 512], P(None, 'tp'), may hold values from -0.25 to 0.25
Outputs:
- token_grad: bfloat16 [16384, 2048], P('ep', 'tp')
- weight_grad: float32 [16384, 2], P('ep')
- gate_grad: bfloat16 [128, 2048, 512], P('ep', None, 'tp')
- up_grad: bfloat16 [128, 2048, 512], P('ep', None, 'tp')
- down_grad: bfloat16 [128, 512, 2048], P('ep', 'tp')
- sharedgate_grad: float32 [2048, 512], P('ep', 'tp')
- sharedup_grad: float32 [2048, 512], P('ep', 'tp')
- shareddown_grad: float32 [2048, 512], P('ep', 'tp')
The draws below stay inside these ranges and needn't reach their ends.
Inputs may be any that keep to these rules, and one draw needn't show every extreme that they name: `routes`: the 2 entries of a token name different experts. Among the 128 tokens of one group no expert is named more than 3 times, and in some groups an expert is named exactly 3 times.
All inputs are finite; a program needn't handle non-finite values.
Results may differ from the reference program's by a relative error of at most 0.007.
Values may be sent and summed in bfloat16 or wider, within the bound.
A program may use at most 128 MiB of HBM per device.

```python
import math
import jax
import jax.numpy as jnp
import numpy as np
from jax import lax

D = 2048
F = 512
FS = 512
TOP_K = 2
TOK_DEV = 128
EXPERTS = 128
TOKENS = 16384
CAP = 3
N_EP = 128
N_TP = 2


def strengthened(result, key, source, target, shards_of, factor):
    def block_of(position):
        return (jnp.arange(result.shape[position]) // (result.shape[position] // shards_of)).reshape((-1,) + (1,) * (result.ndim - 1 - position))

    one_side = jax.random.permutation(key, shards_of)[block_of(target)]
    other_side = (block_of(target) + shards_of // 2) % shards_of
    return jnp.where((block_of(source) == one_side) | (block_of(source) == other_side), factor * result, result)


def block_levels(rng, dims, pieces, smallest, high):
    def one(dim, blocks):
        steps = jax.random.uniform(jax.random.fold_in(jax.random.fold_in(rng, 6), dim), (blocks,), jnp.float32, smallest / len(pieces), high / len(pieces))
        return jnp.repeat(jnp.exp(steps), dims[dim] // blocks).reshape((-1,) + (1,) * (len(dims) - dim - 1))

    factor_of = one(*pieces[0])
    for cut in pieces[1:]:
        factor_of = factor_of * one(*cut)
    return factor_of


def deal_out(stream_key, own, number, rows, number_of, top, most, slope):
    sequence = jax.random.permutation(stream_key, number_of)
    crowded, common = portions_of(number_of, rows * top, most, slope, True), portions_of(number_of, rows * top, most, slope, False)
    places = jnp.arange(number_of)

    def named(lengths, offset_by):
        used = int((lengths > 0).sum())
        fixed = max(1, used // 4)
        moved = fixed + (places - fixed + offset_by * (used - fixed)) % max(1, number_of - fixed)
        return jnp.zeros((number_of,), jnp.int32).at[sequence[jnp.where(places < fixed, places, moved)]].set(jnp.asarray(lengths, jnp.int32))

    lengths = jnp.where(number % 4 == 0, named(crowded, number // 4), named(common, number - number // 4 - 1))
    mixed = jax.random.permutation(jax.random.fold_in(own, 3), number_of)
    source_of, taker = mixed[0:number_of // 2 * 2:2], mixed[1:number_of // 2 * 2:2]
    slack = jnp.minimum(lengths[source_of] - 1, most - lengths[taker]) // 2
    slack = jnp.where((source_of == sequence[0]) | (taker == sequence[0]) | (lengths[taker] == 0), 0, jnp.maximum(slack, 0))
    moved = jax.random.randint(jax.random.fold_in(own, 4), (number_of // 2,), 0, 1 << 20) % (slack + 1)
    lengths = lengths.at[source_of].add(-moved).at[taker].add(moved)
    members = jnp.searchsorted(jnp.cumsum(lengths), jnp.arange(rows * top), side="right").astype(jnp.int32)
    grid = members.reshape(top, rows).T
    grid = grid[jax.random.permutation(jax.random.fold_in(own, 1), rows)]
    offset_by = jax.random.randint(jax.random.fold_in(own, 2), (rows, 1), 0, top)
    return jnp.take_along_axis(grid, (jnp.arange(top)[None, :] + offset_by) % top, axis=1)


def portions_of(number_of, total, limit, skew, full):
    portions = [(1 << 20) // math.isqrt(rank ** skew) + 1 for rank in range(1, number_of + 1)]
    largest = limit if full else min(limit, max(-(-total // number_of), total * portions[0] // sum(portions)))
    least = 1 if total - largest >= number_of - 1 else 0
    given, rest = [largest] + [least] * (number_of - 1), total - largest - least * (number_of - 1)
    while rest > 0:
        movable = [i for i in range(1, number_of) if given[i] < largest] or [i for i in range(1, number_of) if given[i] < limit]
        whole, budget = sum([portions[i] for i in movable]), rest
        for i in movable:
            extra = min(limit - given[i], max(1, budget * portions[i] // whole), rest)
            given[i] = given[i] + extra
            rest = rest - extra
    return np.array(given)


def centred(key, shape, deviation, most, shards=(), kind=jnp.bfloat16):
    entries = jax.random.normal(key, shape, jnp.float32) * deviation
    if len(shards) > 0:
        entries = block_levels(key, shape, shards, -0.22, 0.18) * entries
    return jnp.clip(entries, min=-most, max=most).astype(kind)


def gaussian_with(stream_key, extent, spread, limit, shards, heavy, held_as=jnp.bfloat16):
    entries = spread * jax.random.normal(stream_key, extent, jnp.float32)
    if shards:
        entries = entries * block_levels(stream_key, extent, shards, -0.22, 0.18)
    return jnp.clip(strengthened(entries, jax.random.fold_in(stream_key, 3), *heavy), -limit, limit).astype(held_as)


def setup_inputs(seed: int = 0) -> dict:
    streams_of = jax.random.split(jax.random.key(seed), 11)
    tokens = gaussian_with(streams_of[0], (TOKENS, D), 1.0, 24.0, ((0, 128), (1, 2)), (0, 1, 128, 5.5))
    cotangent = gaussian_with(streams_of[1], (TOKENS, D), 1.0, 24.0, ((0, 128), (1, 2)), (0, 1, 128, 5.5))
    routes_keys = jax.random.split(jax.random.fold_in(streams_of[2], 1), TOKENS // TOK_DEV)
    routes_turns = jax.random.permutation(jax.random.fold_in(streams_of[2], 3), TOKENS // TOK_DEV)
    routes = jax.vmap(lambda own, number: deal_out(jax.random.fold_in(streams_of[2], 2), own, number, TOK_DEV, EXPERTS, TOP_K, CAP, 1))(routes_keys, routes_turns).reshape((TOKENS, TOP_K))
    route_weights = jnp.clip(jnp.exp(math.log(2.5) - 3.218876 * jax.random.uniform(streams_of[3], (TOKENS, TOP_K), jnp.float32) ** block_levels(streams_of[3], (TOKENS, TOP_K), ((0, 128),), -0.2, 0.2)), 0.1, 2.5)
    gate_proj = centred(streams_of[4], (EXPERTS, D, F), D ** -0.5, 0.125, ((0, 128), (2, 2)))
    up_proj = centred(streams_of[5], (EXPERTS, D, F), D ** -0.5, 0.125, ((0, 128), (2, 2)))
    down_proj = centred(streams_of[6], (EXPERTS, F, D), F ** -0.5, 0.25, ((0, 128), (1, 2)))
    shared_gate = centred(streams_of[7], (D, FS), D ** -0.5, 0.125, ((1, 2),))
    shared_up = centred(streams_of[8], (D, FS), D ** -0.5, 0.125, ((1, 2),))
    shared_down = centred(streams_of[9], (D, FS), FS ** -0.5, 0.25, ((1, 2),))
    return dict(tokens=tokens, cotangent=cotangent, routes=routes, route_weights=route_weights, gate_proj=gate_proj, up_proj=up_proj, down_proj=down_proj, shared_gate=shared_gate, shared_up=shared_up, shared_down=shared_down)


def slot_table(routes, experts, capacity):
    assigned = routes.shape[0] * routes.shape[1]
    flat_routes = routes.reshape(assigned).astype(jnp.int32)
    onehot = (flat_routes[:, None] == jnp.arange(experts, dtype=jnp.int32)[None, :]).astype(jnp.int32)
    before = jnp.cumsum(onehot, axis=0) - onehot
    slot_rank = jnp.sum(before * onehot, axis=1).astype(jnp.int32)
    slot_of = (flat_routes * capacity + slot_rank).astype(jnp.int32)
    empty = jnp.full((experts * capacity,), assigned, jnp.int32)
    slot_owner = empty.at[slot_of].set(jnp.arange(assigned, dtype=jnp.int32))
    return slot_of, slot_owner


def silu_parts(preact):
    sigmoid_v = jax.nn.sigmoid(preact)
    return preact * sigmoid_v, sigmoid_v * (1.0 + preact * (1.0 - sigmoid_v))


def rounded(partial_value):
    return lax.optimization_barrier(partial_value.astype(jnp.bfloat16)).astype(jnp.float32)


def contract_rows(left, right):
    return lax.dot_general(left, right, (((0,), (0,)), ((), ())), preferred_element_type=jnp.float32)


def contract_cols(left, right):
    return lax.dot_general(left, right, (((1,), (1,)), ((), ())), preferred_element_type=jnp.float32)


def reference(tokens, cotangent, routes, route_weights, gate_proj, up_proj, down_proj, shared_gate, shared_up, shared_down):
    assigned = TOK_DEV * TOP_K
    row_width = tokens.shape[1]
    block_size = F // N_TP
    slot_of, slot_owner = jax.vmap(lambda device_routes: slot_table(device_routes, EXPERTS, CAP))(
        routes.reshape(N_EP, TOK_DEV, TOP_K))
    filled = slot_owner < assigned
    owner_safe = jnp.minimum(slot_owner, assigned - 1)
    source = jnp.arange(N_EP, dtype=jnp.int32)[:, None]
    token_at = (source * TOK_DEV + owner_safe // TOP_K).astype(jnp.int32)
    assign_at = (source * assigned + owner_safe).astype(jnp.int32)
    flat_weights = route_weights.reshape(N_EP * assigned)
    weight_at = jnp.where(filled, flat_weights[assign_at], jnp.zeros((), jnp.float32))

    def by_expert(layout):
        return jnp.swapaxes(layout.reshape(N_EP, EXPERTS, CAP), 0, 1).reshape(EXPERTS, N_EP * CAP)

    def expert_step(running, inputs):
        input_acc, weight_acc = running
        token_index, assign_index, slot_weights, slot_live, gate_mat, up_mat, down_mat = inputs
        slot_rows = jnp.where(slot_live[:, None], tokens[token_index], jnp.zeros((), jnp.bfloat16))
        slot_cot = (slot_weights[:, None] * cotangent[token_index].astype(jnp.float32)).astype(jnp.bfloat16)
        gate_pre = jnp.dot(slot_rows, gate_mat, preferred_element_type=jnp.float32)
        up_pre = jnp.dot(slot_rows, up_mat, preferred_element_type=jnp.float32)
        gate_act, gate_slope = silu_parts(gate_pre)
        hidden = gate_act * up_pre
        back_grad = contract_cols(slot_cot, down_mat)
        hidden_low = hidden.astype(jnp.bfloat16)
        down_grad = contract_rows(hidden_low, slot_cot).astype(jnp.bfloat16)
        gate_delta = (back_grad * up_pre * gate_slope).astype(jnp.bfloat16)
        up_delta = (back_grad * gate_act).astype(jnp.bfloat16)
        gate_grad = contract_rows(slot_rows, gate_delta).astype(jnp.bfloat16)
        up_grad = contract_rows(slot_rows, up_delta).astype(jnp.bfloat16)
        slot_sum = jnp.zeros((slot_rows.shape[0], row_width), jnp.float32)
        product_sum = jnp.zeros((slot_rows.shape[0],), jnp.float32)
        for block_index in range(N_TP):
            start_col = block_index * block_size
            stop_col = start_col + block_size
            partial_value = contract_cols(gate_delta[:, start_col:stop_col], gate_mat[:, start_col:stop_col])
            partial_value = partial_value + contract_cols(up_delta[:, start_col:stop_col], up_mat[:, start_col:stop_col])
            slot_sum = slot_sum + rounded(partial_value)
            product_sum = product_sum + rounded(jnp.sum(hidden[:, start_col:stop_col] * back_grad[:, start_col:stop_col], axis=1))
        slot_low = rounded(slot_sum)
        product_low = rounded(product_sum)
        input_acc = input_acc.at[token_index].add(jnp.where(slot_live[:, None], slot_low, jnp.zeros((), jnp.float32)))
        weight_acc = weight_acc.at[assign_index].add(jnp.where(slot_live, product_low, jnp.zeros((), jnp.float32)))
        return (input_acc, weight_acc), (gate_grad, up_grad, down_grad)

    start_acc = (jnp.zeros((TOKENS, row_width), jnp.float32), jnp.zeros((TOKENS * TOP_K,), jnp.float32))
    (input_acc, weight_acc), (gate_grad, up_grad, down_grad) = lax.scan(
        expert_step, start_acc,
        (by_expert(token_at), by_expert(assign_at), by_expert(weight_at), by_expert(filled), gate_proj, up_proj, down_proj))

    mix_gate = jnp.dot(tokens, shared_gate, preferred_element_type=jnp.float32)
    mix_up = jnp.dot(tokens, shared_up, preferred_element_type=jnp.float32)
    mix_act, mix_slope = silu_parts(mix_gate)
    mix_hidden = (mix_act * mix_up).astype(jnp.bfloat16)
    mix_back = jnp.dot(cotangent, shared_down, preferred_element_type=jnp.float32)
    mixgrad_gate = (mix_back * mix_up * mix_slope).astype(jnp.bfloat16)
    mixgrad_up = (mix_back * mix_act).astype(jnp.bfloat16)
    mix_block = FS // N_TP
    mix_input = jnp.zeros((TOKENS, row_width), jnp.float32)
    for block_index in range(N_TP):
        start_col = block_index * mix_block
        stop_col = start_col + mix_block
        partial_value = contract_cols(mixgrad_gate[:, start_col:stop_col], shared_gate[:, start_col:stop_col])
        partial_value = partial_value + contract_cols(mixgrad_up[:, start_col:stop_col], shared_up[:, start_col:stop_col])
        mix_input = mix_input + rounded(partial_value)
    token_grad = (mix_input + input_acc).astype(jnp.bfloat16)
    weight_grad = weight_acc.reshape(TOKENS, TOP_K) / route_weights
    sharedgate_grad = contract_rows(tokens, mixgrad_gate)
    sharedup_grad = contract_rows(tokens, mixgrad_up)
    shareddown_grad = contract_rows(cotangent, mix_hidden)
    return (token_grad, weight_grad, gate_grad, up_grad, down_grad, sharedgate_grad, sharedup_grad, shareddown_grad)
```

```python
import math

import jax
import jax.numpy as jnp
from jax import lax
from jax.experimental import pallas as pl
from jax.experimental.pallas import tpu as pltpu
from jax.sharding import Mesh
from jax.sharding import PartitionSpec as P

EP = ("ep_0", "ep_1", "ep_2")


def sent_together(arrays, axis, dim, along):
    widths = [a.shape[along] for a in arrays]
    both = jnp.concatenate(arrays, axis=along)
    filled = lax.all_gather(both, axis, axis=dim, tiled=True)
    return tuple(jnp.split(filled, [sum(widths[:k]) for k in range(1, len(widths))], axis=along))


def split_up(shard, dim, peers):
    lengths = shard.shape
    blocks = shard.reshape(*lengths[:dim], peers, lengths[dim] // peers, *lengths[dim + 1 :])
    return jnp.moveaxis(blocks, dim, 0)


def sum_at_owner(shard, axis, dim):
    peers = lax.axis_size(axis)
    blocks = lax.all_to_all(split_up(shard, dim, peers), axis, 0, 0, tiled=True)
    return jnp.sum(blocks.astype(jnp.float32), axis=0)


def side_by_side_2(arrays, axis, dim, along):
    both = jnp.concatenate(arrays, axis=along)
    filled, at, outs = (sum_at_owner(both, axis, dim), 0, [])
    for a in arrays:
        outs.append(lax.slice_in_dim(filled, at, at + a.shape[along], axis=along))
        at += a.shape[along]
    return tuple(outs)


def direct_kernel(send, recv, send_sem, recv_sem):
    z, y, x, c = (lax.axis_index(n) for n in ("ep_0", "ep_1", "ep_2", "tp"))
    nz, ny, nx = (lax.axis_size(n) for n in ("ep_0", "ep_1", "ep_2"))
    count = nz * ny * nx
    me = (z * ny + y) * nx + x

    def peer(step):
        pz = lax.rem(z + step // (ny * nx), nz)
        py = lax.rem(y + lax.rem(step // nx, ny), ny)
        px = lax.rem(x + lax.rem(step, nx), nx)
        return (pz * ny + py) * nx + px, (pz, py, px, c)

    barrier = pltpu.get_barrier_semaphore()

    def greet(step, carry):
        pl.semaphore_signal(
            barrier, inc=1, device_id=peer(step)[1], device_id_type=pl.DeviceIdType.MESH
        )
        return carry

    lax.fori_loop(1, count, greet, 0)
    recv[me] = send[me]
    pl.semaphore_wait(barrier, count - 1)

    def launch(step, carry):
        index, device = peer(step)
        pltpu.make_async_remote_copy(
            src_ref=send.at[index],
            dst_ref=recv.at[me],
            send_sem=send_sem,
            recv_sem=recv_sem,
            device_id=device,
            device_id_type=pl.DeviceIdType.MESH,
        ).start()
        return carry

    lax.fori_loop(1, count, launch, 0)
    rest = pl.ds(0, count - 1)
    pltpu.make_async_copy(send.at[rest], send.at[rest], send_sem).wait()
    pltpu.make_async_copy(recv.at[rest], recv.at[rest], recv_sem).wait()


def direct_exchange(blocks, collective_id):
    return pl.pallas_call(
        direct_kernel,
        out_shape=jax.ShapeDtypeStruct(blocks.shape, blocks.dtype),
        in_specs=[pl.BlockSpec(memory_space=pltpu.VMEM)],
        out_specs=pl.BlockSpec(memory_space=pltpu.VMEM),
        scratch_shapes=[pltpu.SemaphoreType.DMA, pltpu.SemaphoreType.DMA],
        compiler_params=pltpu.CompilerParams(
            collective_id=collective_id, has_side_effects=True, vmem_limit_bytes=16 << 20
        ),
        name=f"direct_{collective_id}",
    )(blocks)


def own_rows(running, axes):
    sizes = [lax.axis_size(axis) for axis in axes]
    total = math.prod(sizes)
    rows, cols = running.shape
    blocks = running.astype(jnp.bfloat16).reshape(*sizes, rows // total, cols)
    running = blocks.transpose(2, 1, 0, 3, 4).reshape(rows, cols)
    for axis in axes[::-1]:
        running = lax.psum_scatter(running, axis, scatter_dimension=0, tiled=True)
    return running.astype(jnp.float32)


def slot_table(routes, experts, capacity):
    assigned = routes.shape[0] * routes.shape[1]
    flat_routes = routes.reshape(assigned)
    onehot = (flat_routes[:, None] == jnp.arange(experts, dtype=jnp.int32)[None, :]).astype(
        jnp.int32
    )
    before = jnp.cumsum(onehot, axis=0) - onehot
    slot_rank = jnp.sum(before * onehot, axis=1)
    slot_of = flat_routes * capacity + slot_rank
    empty = jnp.full((experts * capacity,), assigned, jnp.int32)
    slot_owner = empty.at[slot_of].set(jnp.arange(assigned, dtype=jnp.int32))
    return (slot_of, slot_owner)


def silu_parts(preact):
    sigmoid_v = jax.nn.sigmoid(preact)
    return (preact * sigmoid_v, sigmoid_v * (1.0 + preact * (1.0 - sigmoid_v)))


def rounded(partial_value):
    return lax.optimization_barrier(partial_value.astype(jnp.bfloat16)).astype(jnp.float32)


def contract_rows(left, right):
    return lax.dot_general(
        left, right, (((0,), (0,)), ((), ())), preferred_element_type=jnp.float32
    )


def contract_cols(left, right):
    return lax.dot_general(
        left, right, (((1,), (1,)), ((), ())), preferred_element_type=jnp.float32
    )


def per_device(
    tokens,
    cotangent,
    routes,
    route_weights,
    gate_proj,
    up_proj,
    down_proj,
    shared_gate,
    shared_up,
    shared_down,
):
    groups = lax.axis_size(EP)
    halves = lax.axis_size("tp")
    local_count = gate_proj.shape[0]
    experts = groups * local_count
    token_rows, top = routes.shape
    assigned = token_rows * top
    capacity = assigned // experts + assigned // (2 * experts)
    per_peer = local_count * capacity
    whole_rows, whole_cot = sent_together((tokens, cotangent), "tp", 1, 0)
    slot_of, slot_owner = slot_table(routes, experts, capacity)
    filled = slot_owner < assigned
    owner_safe = jnp.minimum(slot_owner, assigned - 1)
    slot_token = owner_safe // top
    slot_weight = jnp.where(
        filled, route_weights.reshape(assigned)[owner_safe], jnp.zeros((), jnp.float32)
    )
    col_count = tokens.shape[1]
    packed_rows = jnp.where(filled[:, None], tokens[slot_token], jnp.zeros((), jnp.bfloat16))
    packed_cot = (slot_weight[:, None] * cotangent[slot_token].astype(jnp.float32)).astype(
        jnp.bfloat16
    )
    sent_rows = packed_rows.reshape(groups, per_peer, col_count)
    sent_cot = packed_cot.reshape(groups, per_peer, col_count)
    both = jnp.concatenate((sent_rows, sent_cot), axis=1)
    arrived = direct_exchange(both.reshape(groups, -1, 128), 0)
    arrived = arrived.reshape(groups, 2 * per_peer, col_count)
    half_rows, half_cot = arrived[:, :per_peer], arrived[:, per_peer:]
    got_rows, got_cot = sent_together((half_rows, half_cot), "tp", 2, 0)

    def by_expert(layout):
        return jnp.swapaxes(layout.reshape(groups, local_count, capacity, -1), 0, 1).reshape(
            local_count, groups * capacity, -1
        )

    def by_peer(layout):
        return jnp.swapaxes(layout.reshape(local_count, groups, capacity, -1), 0, 1).reshape(
            groups * per_peer, -1
        )

    slot_rows = by_expert(got_rows)
    slot_cot = by_expert(got_cot)
    gate_pre = jnp.einsum("erd,edf->erf", slot_rows, gate_proj, preferred_element_type=jnp.float32)
    up_pre = jnp.einsum("erd,edf->erf", slot_rows, up_proj, preferred_element_type=jnp.float32)
    gate_act, gate_slope = silu_parts(gate_pre)
    hidden = gate_act * up_pre
    back_grad = jnp.einsum("erd,efd->erf", slot_cot, down_proj, preferred_element_type=jnp.float32)
    product = jnp.sum(hidden * back_grad, axis=2, keepdims=True)
    hidden_low = hidden.astype(jnp.bfloat16)
    down_grad = jnp.einsum(
        "erf,erd->efd", hidden_low, slot_cot, preferred_element_type=jnp.float32
    ).astype(jnp.bfloat16)
    gate_delta = (back_grad * up_pre * gate_slope).astype(jnp.bfloat16)
    up_delta = (back_grad * gate_act).astype(jnp.bfloat16)
    gate_grad = jnp.einsum(
        "erd,erf->edf", slot_rows, gate_delta, preferred_element_type=jnp.float32
    ).astype(jnp.bfloat16)
    up_grad = jnp.einsum(
        "erd,erf->edf", slot_rows, up_delta, preferred_element_type=jnp.float32
    ).astype(jnp.bfloat16)
    input_part = jnp.einsum(
        "erf,edf->erd", gate_delta, gate_proj, preferred_element_type=jnp.float32
    )
    input_part = input_part + jnp.einsum(
        "erf,edf->erd", up_delta, up_proj, preferred_element_type=jnp.float32
    )
    mix_gate = jnp.dot(whole_rows, shared_gate, preferred_element_type=jnp.float32)
    mix_up = jnp.dot(whole_rows, shared_up, preferred_element_type=jnp.float32)
    mix_act, mix_slope = silu_parts(mix_gate)
    mix_hidden = (mix_act * mix_up).astype(jnp.bfloat16)
    mix_back = jnp.dot(whole_cot, shared_down, preferred_element_type=jnp.float32)
    mixgrad_gate = (mix_back * mix_up * mix_slope).astype(jnp.bfloat16)
    mixgrad_up = (mix_back * mix_act).astype(jnp.bfloat16)
    mix_partial = contract_cols(mixgrad_gate, shared_gate) + contract_cols(mixgrad_up, shared_up)
    product_cols = jnp.broadcast_to(by_peer(product), (groups * per_peer, halves))
    slot_sum, mix_sum, product_sum = (
        *side_by_side_2(
            (
                rounded(by_peer(input_part)).astype(jnp.bfloat16),
                rounded(mix_partial).astype(jnp.bfloat16),
            ),
            "tp",
            1,
            0,
        ),
        sum_at_owner(rounded(product_cols).astype(jnp.bfloat16), "tp", 1),
    )
    back_rows = slot_sum.astype(jnp.bfloat16).reshape(groups, per_peer, -1)
    back_prod = product_sum.astype(jnp.bfloat16).reshape(groups, per_peer)
    tail = jnp.pad(back_prod[:, None, :], ((0, 0), (0, 7), (0, 128 - per_peer)))
    leaving = jnp.concatenate((back_rows.reshape(groups, -1, 128), tail), axis=1)
    home = direct_exchange(leaving, 1)
    home_rows = home[:, : per_peer * 8].reshape(groups, per_peer, -1)
    home_prod = home[:, per_peer * 8, :per_peer]
    per_slot = home_rows.reshape(experts * capacity, -1)[slot_of].astype(jnp.float32)
    token_grad = (mix_sum + jnp.sum(per_slot.reshape(token_rows, top, -1), axis=1)).astype(
        jnp.bfloat16
    )
    slot_product = home_prod.reshape(experts * capacity)[slot_of].astype(jnp.float32)
    weight_grad = slot_product.reshape(token_rows, top) / route_weights
    mix_cols = mixgrad_gate.shape[1]
    stacked = own_rows(
        jnp.concatenate(
            [
                contract_rows(whole_rows, mixgrad_gate),
                contract_rows(whole_rows, mixgrad_up),
                contract_rows(whole_cot, mix_hidden),
            ],
            axis=1,
        ),
        EP,
    )
    return (
        token_grad,
        weight_grad,
        gate_grad,
        up_grad,
        down_grad,
        stacked[:, :mix_cols],
        stacked[:, mix_cols : 2 * mix_cols],
        stacked[:, 2 * mix_cols :],
    )


def solution(mesh):
    split = Mesh(mesh.devices.reshape(8, 4, 4, mesh.shape["tp"]), ("ep_0", "ep_1", "ep_2", "tp"))
    placed = (
        P(EP, "tp"),
        P(EP, "tp"),
        P(EP, None),
        P(EP, None),
        P(EP, None, "tp"),
        P(EP, None, "tp"),
        P(EP, "tp", None),
        P(None, "tp"),
        P(None, "tp"),
        P(None, "tp"),
    )
    return jax.shard_map(
        per_device,
        mesh=split,
        in_specs=placed,
        out_specs=(
            P(EP, "tp"),
            P(EP, None),
            P(EP, None, "tp"),
            P(EP, None, "tp"),
            P(EP, "tp", None),
            P(EP, "tp"),
            P(EP, "tp"),
            P(EP, "tp"),
        ),
        check_vma=False,
    )
```

```python
import jax
import jax.numpy as jnp
from jax import lax
from jax.experimental import pallas as pl
from jax.experimental.pallas import tpu as pltpu
from jax.sharding import Mesh
from jax.sharding import PartitionSpec as P

EP = ("ep_0", "ep_1", "ep_2")
BF = jnp.bfloat16
F32 = jnp.float32
CAP = 3
LANES = 128


def dot(left, right, dims):
    return lax.dot_general(left, right, ((dims[:1], dims[1:]), ((), ())), preferred_element_type=F32)


def silu_parts(preact):
    sigmoid_v = jax.nn.sigmoid(preact)
    return (preact * sigmoid_v, sigmoid_v * (1.0 + preact * (1.0 - sigmoid_v)))


def fused_kernel(
    nz, ny, nx,
    tokens, cotangent, routes, route_weights, gate_proj, up_proj, down_proj,
    shared_gate, shared_up, shared_down,
    token_grad, weight_grad, gate_grad, up_grad, down_grad, sgate_grad, sup_grad, sdown_grad,
    wtok, wcot, wgu, wd, sgu, sd,
    onehot, wide, wide2, send1, recv1, fwd1, rows, cots,
    pre, back, hidden, delta, part, part_in, prod, prod_in, prod_out, prod_home,
    send2, recv2, home, mix, mix_in, mix_sum, smix, shid,
    grad_gu, grad_d, ga, gb, ra1, rb1, sa2, sb2, ra2, rb2, sa3, sb3, ra3, rb3,
    load_sem, tp_send, tp_recv, s1_sem, r1_sem, f_send, f_recv, p_send, p_recv,
    m_send, m_recv, s2_sem, r2_sem, q_send, q_recv, rs_send, rs_recv, out_sem,
):
    z, y, x, c = (lax.axis_index(n) for n in EP + ("tp",))
    chips = nz * ny * nx
    plane = ny * nx
    me = (z * ny + y) * nx + x
    toks, half = tokens.shape
    width = 2 * half
    hid = wd.shape[0]
    chunks = half // LANES
    q1 = 2 * CAP * chunks
    q2 = CAP * chunks
    first = pl.ds(pl.multiple_of(c * half, LANES), half)
    second = pl.ds(pl.multiple_of((1 - c) * half, LANES), half)
    partner = (z, y, x, 1 - c)

    def remote(src, dst, send_sem, recv_sem, device):
        return pltpu.make_async_remote_copy(
            src_ref=src, dst_ref=dst, send_sem=send_sem, recv_sem=recv_sem,
            device_id=device, device_id_type=pl.DeviceIdType.MESH,
        )

    def await_bytes(ref, sem):
        pltpu.make_async_copy(ref, ref, sem).wait()

    def peer(step):
        pz = lax.rem(z + step // plane, nz)
        py = lax.rem(y + lax.rem(step // nx, ny), ny)
        px = lax.rem(x + lax.rem(step, nx), nx)
        return (pz * ny + py) * nx + px, (pz, py, px, c)

    loads = [
        pltpu.make_async_copy(src, dst, load_sem.at[i])
        for i, (src, dst) in enumerate(
            (
                (tokens, wtok.at[:, :half]),
                (cotangent, wcot.at[:, :half]),
                (shared_gate.at[first], sgu.at[:half, :hid]),
                (shared_gate.at[second], sgu.at[half:, :hid]),
                (shared_up.at[first], sgu.at[:half, hid:]),
                (shared_up.at[second], sgu.at[half:, hid:]),
                (shared_down.at[first], sd.at[:half]),
                (shared_down.at[second], sd.at[half:]),
                (gate_proj.at[first], wgu.at[:half, :hid]),
                (gate_proj.at[second], wgu.at[half:, :hid]),
                (up_proj.at[first], wgu.at[:half, hid:]),
                (up_proj.at[second], wgu.at[half:, hid:]),
                (down_proj.at[:, first], wd.at[:, :half]),
                (down_proj.at[:, second], wd.at[:, half:]),
            )
        )
    ]
    for copy in loads:
        copy.start()

    barrier = pltpu.get_barrier_semaphore()
    pl.semaphore_signal(barrier, inc=1, device_id=partner, device_id_type=pl.DeviceIdType.MESH)

    def greet(step, carry):
        pl.semaphore_signal(
            barrier, inc=1, device_id=peer(step)[1], device_id_type=pl.DeviceIdType.MESH
        )
        return carry

    lax.fori_loop(1, chips, greet, 0)

    lane = lax.broadcasted_iota(jnp.int32, (toks, chips), 1)
    sub = lax.broadcasted_iota(jnp.int32, (toks, chips), 0)
    picks = [routes[:, k : k + 1] == lane for k in range(2)]
    named = picks[0].astype(F32) + picks[1].astype(F32)
    earlier = dot((lane < sub).astype(BF), named.astype(BF), (1, 0))
    weight_of = jnp.where(picks[0], route_weights[:, 0:1], 0.0) + jnp.where(
        picks[1], route_weights[:, 1:2], 0.0
    )
    columns = []
    for r in range(CAP):
        held = jnp.where(earlier == float(r), named, 0.0)
        onehot[:, r * chips : (r + 1) * chips] = held.astype(BF)
        row = jnp.sum(held * weight_of, axis=0, keepdims=True)
        columns.append(jnp.sum(jnp.where(lane == sub, row, 0.0), axis=1, keepdims=True))

    loads[0].wait()
    loads[1].wait()
    for r in range(CAP):
        pick = onehot[:, r * chips : (r + 1) * chips]
        for t, source in enumerate((wtok, wcot)):
            chosen = dot(pick, source[:, :half], (0, 0))
            if t == 1:
                chosen = columns[r] * chosen
            for k in range(chunks):
                wide[pl.ds((t * CAP + r) * chunks + k, chips, stride=q1), :] = chosen[
                    :, k * LANES : (k + 1) * LANES
                ]

    def narrow(i, carry):
        block = wide[pl.ds(pl.multiple_of(i * plane * q1, plane * q1), plane * q1), :]
        send1[pl.ds(i * plane, plane)] = block.reshape(plane, q1, LANES).astype(BF)
        return carry

    lax.fori_loop(0, nz, narrow, 0)
    recv1[me] = send1[me]

    pl.semaphore_wait(barrier, chips)

    trade = [
        remote(ref.at[:, :half], ref.at[:, half:], tp_send.at[i], tp_recv.at[i], partner)
        for i, ref in enumerate((wtok, wcot))
    ]
    for copy in trade:
        copy.start()

    def launch(step, carry):
        index, device = peer(step)
        remote(send1.at[index], recv1.at[me], s1_sem, r1_sem.at[step // plane], device).start()
        return carry

    lax.fori_loop(1, chips, launch, 0)

    for copy in loads[2:8]:
        copy.wait()
    for copy in trade:
        copy.wait()
    smix[...] = dot(wtok[...], sgu[...], (1, 0))
    mix_back = dot(wcot[...], sd[...], (1, 0))
    mix_act, mix_slope = silu_parts(smix[:, :hid])
    mix_up = smix[:, hid:]
    shid[:, 2 * hid :] = (mix_act * mix_up).astype(BF)
    shid[:, :hid] = (mix_back * mix_up * mix_slope).astype(BF)
    shid[:, hid : 2 * hid] = (mix_back * mix_act).astype(BF)

    zrows = width // nz
    zhalf = nz // 2
    cut = ga.shape[-1]

    def shared_terms(i, carry):
        at = pl.ds(pl.multiple_of(i * zrows, LANES), zrows)
        block = lax.rem(i + c * zhalf, nz)
        one = dot(wtok[:, at], shid[:, : 2 * hid], (0, 0)).astype(BF)
        two = dot(wcot[:, at], shid[:, 2 * hid :], (0, 0)).astype(BF)
        ga[block] = one[:, :cut].reshape(ny, nx, zrows // plane, cut)
        gb[block, :, :, :, : 2 * hid - cut] = one[:, cut:].reshape(
            ny, nx, zrows // plane, 2 * hid - cut
        )
        gb[block, :, :, :, 2 * hid - cut :] = two.reshape(ny, nx, zrows // plane, hid)
        return carry

    lax.fori_loop(0, nz, shared_terms, 0)

    mix[...] = dot(shid[:, : 2 * hid], sgu[half:, :], (1, 1)).astype(BF)
    trade_mix = remote(mix, mix_in, m_send, m_recv, partner)
    trade_mix.start()
    for d in range(1, nx):
        px = lax.rem(x + d, nx)
        remote(ga.at[:, :, px], ra1.at[d - 1], rs_send.at[0], rs_recv.at[0], (z, y, px, c)).start()
    for d in range(1, ny):
        py = lax.rem(y + d, ny)
        remote(gb.at[:, py], rb1.at[d - 1], rs_send.at[1], rs_recv.at[1], (z, py, x, c)).start()
    mix_sum[...] = dot(shid[:, : 2 * hid], sgu[:half, :], (1, 1)).astype(BF).astype(F32)

    def arrive(dz, carry):
        zs = lax.rem(z - dz + nz, nz)
        group = pl.ds(zs * plane, plane)

        @pl.when(dz == 0)
        def _():
            await_bytes(recv1.at[pl.ds(0, plane - 1)], r1_sem.at[0])

        @pl.when(dz != 0)
        def _():
            await_bytes(recv1.at[pl.ds(0, plane)], r1_sem.at[dz])

        remote(recv1.at[group], fwd1.at[group], f_send, f_recv.at[dz], partner).start()
        wide[pl.ds(pl.multiple_of(zs * plane * q1, plane * q1), plane * q1), :] = (
            recv1[group].astype(F32).reshape(plane * q1, LANES)
        )
        return carry

    lax.fori_loop(0, nz, arrive, 0)

    def arrive_other(dz, carry):
        zs = lax.rem(z - dz + nz, nz)
        group = pl.ds(zs * plane, plane)
        await_bytes(fwd1.at[pl.ds(0, plane)], f_recv.at[dz])
        wide2[pl.ds(pl.multiple_of(zs * plane * q1, plane * q1), plane * q1), :] = (
            fwd1[group].astype(F32).reshape(plane * q1, LANES)
        )
        return carry

    def spread(source, base):
        for t, target in enumerate((rows, cots)):
            for r in range(CAP):
                for k in range(chunks):
                    target[
                        r * chips : (r + 1) * chips, base + k * LANES : base + (k + 1) * LANES
                    ] = source[
                        pl.ds((t * CAP + r) * chunks + k, chips, stride=q1), :
                    ].astype(BF)

    spread(wide, 0)
    lax.fori_loop(0, nz, arrive_other, 0)
    spread(wide2, half)

    for copy in loads[8:]:
        copy.wait()
    pre[...] = dot(rows[...], wgu[...], (1, 0))
    back[...] = dot(cots[...], wd[...], (1, 1))

    for r in range(CAP):
        at = pl.ds(r * chips, chips)
        gate_act, gate_slope = silu_parts(pre[at, :hid])
        up_pre = pre[at, hid:]
        grad = back[at, :]
        value = gate_act * up_pre
        hidden[at, :] = value.astype(BF)
        delta[at, :hid] = (grad * up_pre * gate_slope).astype(BF)
        delta[at, hid:] = (grad * gate_act).astype(BF)
        total = jnp.sum(value * grad, axis=1, keepdims=True)
        prod[at, :] = jnp.broadcast_to(total, (chips, LANES)).astype(BF)

    part[...] = dot(delta[...], wgu[half:, :], (1, 1)).astype(BF)
    trade_part = remote(part, part_in, p_send.at[0], p_recv.at[0], partner)
    trade_prod = remote(prod, prod_in, p_send.at[1], p_recv.at[1], partner)
    trade_part.start()
    trade_prod.start()
    own = dot(delta[...], wgu[:half, :], (1, 1)).astype(BF)
    trade_part.wait()
    trade_prod.wait()
    summed = own.astype(F32) + part_in[...].astype(F32)
    for r in range(CAP):
        for k in range(chunks):
            wide[pl.ds(r * chunks + k, chips, stride=q2), :] = summed[
                r * chips : (r + 1) * chips, k * LANES : (k + 1) * LANES
            ]

    def narrow_back(i, carry):
        block = wide[pl.ds(pl.multiple_of(i * plane * q2, plane * q2), plane * q2), :]
        send2[pl.ds(i * plane, plane)] = block.reshape(plane, q2, LANES).astype(BF)
        return carry

    lax.fori_loop(0, nz, narrow_back, 0)
    products = prod[...].astype(F32) + prod_in[...].astype(F32)
    packed = jnp.where(
        lane == 0,
        products[:chips],
        jnp.where(lane == 1, products[chips : 2 * chips], products[2 * chips :]),
    )
    prod_out[:, 0, :] = packed.astype(BF).astype(F32)
    recv2[me] = send2[me]
    prod_home[me] = prod_out[me]

    def give_back(step, carry):
        index, device = peer(step)
        remote(send2.at[index], recv2.at[me], s2_sem, r2_sem, device).start()
        remote(prod_out.at[index], prod_home.at[me], q_send, q_recv, device).start()
        return carry

    lax.fori_loop(1, chips, give_back, 0)

    await_bytes(ra1, rs_recv.at[0])
    await_bytes(rb1, rs_recv.at[1])

    def first_sum(i, carry):
        total = ga[i, :, x].astype(F32)
        other = gb[i, y].astype(F32)
        for d in range(nx - 1):
            total = total + ra1[d, i].astype(F32)
        for d in range(ny - 1):
            other = other + rb1[d, i].astype(F32)
        sa2[i] = total.astype(BF)
        sb2[i] = other.astype(BF)
        return carry

    lax.fori_loop(0, nz, first_sum, 0)
    for d in range(1, ny):
        py = lax.rem(y + d, ny)
        remote(sa2.at[:, py], ra2.at[d - 1], rs_send.at[2], rs_recv.at[2], (z, py, x, c)).start()
    for d in range(1, nx):
        px = lax.rem(x + d, nx)
        remote(sb2.at[:, px], rb2.at[d - 1], rs_send.at[3], rs_recv.at[3], (z, y, px, c)).start()

    def expert_terms(i, carry):
        at = pl.ds(pl.multiple_of(i * zrows, LANES), zrows)
        both = dot(rows[:, at], delta[...], (0, 0)).astype(BF)
        grad_gu[0, at, :] = both[:, :hid]
        grad_gu[1, at, :] = both[:, hid:]
        grad_d[:, at] = dot(hidden[...], cots[:, at], (0, 0)).astype(BF)
        return carry

    lax.fori_loop(0, nz, expert_terms, 0)
    stores = [
        pltpu.make_async_copy(src, dst, out_sem.at[i])
        for i, (src, dst) in enumerate(
            (
                (grad_gu.at[0, :half], gate_grad.at[first]),
                (grad_gu.at[0, half:], gate_grad.at[second]),
                (grad_gu.at[1, :half], up_grad.at[first]),
                (grad_gu.at[1, half:], up_grad.at[second]),
                (grad_d.at[:, :half], down_grad.at[:, first]),
                (grad_d.at[:, half:], down_grad.at[:, second]),
            )
        )
    ]
    for copy in stores:
        copy.start()

    await_bytes(ra2, rs_recv.at[2])
    await_bytes(rb2, rs_recv.at[3])

    def second_sum(i, carry):
        total = sa2[i, y].astype(F32)
        other = sb2[i, x].astype(F32)
        for d in range(ny - 1):
            total = total + ra2[d, i].astype(F32)
        for d in range(nx - 1):
            other = other + rb2[d, i].astype(F32)
        sa3[i] = total.astype(BF)
        sb3[i] = other.astype(BF)
        return carry

    lax.fori_loop(0, nz, second_sum, 0)
    for d in range(1, nz):
        pz = lax.rem(z + d, nz)
        remote(sa3.at[pz], ra3.at[d - 1], rs_send.at[4], rs_recv.at[4], (pz, y, x, c)).start()
        remote(sb3.at[pz], rb3.at[d - 1], rs_send.at[5], rs_recv.at[5], (pz, y, x, c)).start()
    trade_mix.wait()
    mix_sum[...] = mix_sum[...] + mix_in[...].astype(F32)
    await_bytes(ra3, rs_recv.at[4])
    await_bytes(rb3, rs_recv.at[5])
    total = sa3[z].astype(F32)
    other = sb3[z].astype(F32)
    for d in range(nz - 1):
        total = total + ra3[d].astype(F32)
        other = other + rb3[d].astype(F32)
    sgate_grad[...] = total[:, :hid]
    sup_grad[:, : cut - hid] = total[:, hid:]
    sup_grad[:, cut - hid :] = other[:, : 2 * hid - cut]
    sdown_grad[...] = other[:, 2 * hid - cut :]

    await_bytes(prod_home.at[pl.ds(0, chips - 1)], q_recv)
    held = onehot[...]
    seen = prod_home[:, 0, :]
    ranked = [jnp.where(lane == r, seen, 0.0).astype(BF) for r in range(CAP)]
    for k in range(2):
        mine = jnp.zeros((toks, LANES), F32)
        for r in range(CAP):
            chosen = jnp.where(picks[k], held[:, r * chips : (r + 1) * chips].astype(F32), 0.0)
            mine = mine + dot(chosen.astype(BF), ranked[r], (1, 0))
        weight_grad[:, k : k + 1] = (
            jnp.sum(mine, axis=1, keepdims=True) / route_weights[:, k : k + 1]
        )
    await_bytes(recv2.at[pl.ds(0, chips - 1)], r2_sem)
    wide[pl.ds(0, chips * q2), :] = recv2[...].astype(F32).reshape(chips * q2, LANES)
    for r in range(CAP):
        for k in range(chunks):
            home[r * chips : (r + 1) * chips, k * LANES : (k + 1) * LANES] = wide[
                pl.ds(r * chunks + k, chips, stride=q2), :
            ].astype(BF)
    token_grad[...] = (mix_sum[...] + dot(held, home[...], (1, 0))).astype(BF)

    await_bytes(send1.at[pl.ds(0, chips - 1)], s1_sem)
    await_bytes(fwd1, f_send)
    await_bytes(send2.at[pl.ds(0, chips - 1)], s2_sem)
    await_bytes(prod_out.at[pl.ds(0, chips - 1)], q_send)
    for i, ref in enumerate((ra1, rb1, ra2, rb2, ra3, rb3)):
        await_bytes(ref, rs_send.at[i])
    for copy in stores:
        copy.wait()


def per_device(
    tokens, cotangent, routes, route_weights, gate_proj, up_proj, down_proj,
    shared_gate, shared_up, shared_down,
):
    nz, ny, nx = (lax.axis_size(n) for n in EP)
    chips = nz * ny * nx
    toks, half = tokens.shape
    width = 2 * half
    hid = gate_proj.shape[2]
    slots = CAP * chips
    q1, q2 = 2 * CAP * half // LANES, CAP * half // LANES
    rblk = width // chips
    cut = 3 * hid // 2
    hbm = pl.BlockSpec(memory_space=pl.ANY)
    vmem = pl.BlockSpec(memory_space=pltpu.VMEM)
    dma = pltpu.SemaphoreType.DMA

    def kernel(*refs):
        fused_kernel(nz, ny, nx, *refs)

    outs = pl.pallas_call(
        kernel,
        out_shape=[
            jax.ShapeDtypeStruct((toks, half), BF),
            jax.ShapeDtypeStruct((toks, 2), F32),
            jax.ShapeDtypeStruct((width, hid), BF),
            jax.ShapeDtypeStruct((width, hid), BF),
            jax.ShapeDtypeStruct((hid, width), BF),
            jax.ShapeDtypeStruct((rblk, hid), F32),
            jax.ShapeDtypeStruct((rblk, hid), F32),
            jax.ShapeDtypeStruct((rblk, hid), F32),
        ],
        in_specs=[hbm, hbm, vmem, vmem] + [hbm] * 6,
        out_specs=[vmem, vmem, hbm, hbm, hbm, vmem, vmem, vmem],
        scratch_shapes=[
            pltpu.VMEM((toks, width), BF),
            pltpu.VMEM((toks, width), BF),
            pltpu.VMEM((width, 2 * hid), BF),
            pltpu.VMEM((hid, width), BF),
            pltpu.VMEM((width, 2 * hid), BF),
            pltpu.VMEM((width, hid), BF),
            pltpu.VMEM((toks, slots), BF),
            pltpu.VMEM((chips * q1, LANES), F32),
            pltpu.VMEM((chips * q1, LANES), F32),
            pltpu.VMEM((chips, q1, LANES), BF),
            pltpu.VMEM((chips, q1, LANES), BF),
            pltpu.VMEM((chips, q1, LANES), BF),
            pltpu.VMEM((slots, width), BF),
            pltpu.VMEM((slots, width), BF),
            pltpu.VMEM((slots, 2 * hid), F32),
            pltpu.VMEM((slots, hid), F32),
            pltpu.VMEM((slots, hid), BF),
            pltpu.VMEM((slots, 2 * hid), BF),
            pltpu.VMEM((slots, half), BF),
            pltpu.VMEM((slots, half), BF),
            pltpu.VMEM((slots, LANES), BF),
            pltpu.VMEM((slots, LANES), BF),
            pltpu.VMEM((chips, 1, LANES), F32),
            pltpu.VMEM((chips, 1, LANES), F32),
            pltpu.VMEM((chips, q2, LANES), BF),
            pltpu.VMEM((chips, q2, LANES), BF),
            pltpu.VMEM((slots, half), BF),
            pltpu.VMEM((toks, half), BF),
            pltpu.VMEM((toks, half), BF),
            pltpu.VMEM((toks, half), F32),
            pltpu.VMEM((toks, 2 * hid), F32),
            pltpu.VMEM((toks, 3 * hid), BF),
            pltpu.VMEM((2, width, hid), BF),
            pltpu.VMEM((hid, width), BF),
            pltpu.VMEM((nz, ny, nx, rblk, cut), BF),
            pltpu.VMEM((nz, ny, nx, rblk, cut), BF),
            pltpu.VMEM((nx - 1, nz, ny, rblk, cut), BF),
            pltpu.VMEM((ny - 1, nz, nx, rblk, cut), BF),
            pltpu.VMEM((nz, ny, rblk, cut), BF),
            pltpu.VMEM((nz, nx, rblk, cut), BF),
            pltpu.VMEM((ny - 1, nz, rblk, cut), BF),
            pltpu.VMEM((nx - 1, nz, rblk, cut), BF),
            pltpu.VMEM((nz, rblk, cut), BF),
            pltpu.VMEM((nz, rblk, cut), BF),
            pltpu.VMEM((nz - 1, rblk, cut), BF),
            pltpu.VMEM((nz - 1, rblk, cut), BF),
            dma((14,)),
            dma((2,)),
            dma((2,)),
            dma,
            dma((nz,)),
            dma,
            dma((nz,)),
            dma((2,)),
            dma((2,)),
            dma,
            dma,
            dma,
            dma,
            dma,
            dma,
            dma((6,)),
            dma((6,)),
            dma((6,)),
        ],
        compiler_params=pltpu.CompilerParams(
            collective_id=0, has_side_effects=True, vmem_limit_bytes=62 << 20
        ),
        name="fused",
    )(
        tokens, cotangent, routes, route_weights,
        gate_proj[0], up_proj[0], down_proj[0], shared_gate, shared_up, shared_down,
    )
    outs = list(outs)
    for i in (2, 3, 4):
        outs[i] = outs[i][None]
    return tuple(outs)


def solution(mesh):
    split = Mesh(mesh.devices.reshape(8, 4, 4, mesh.shape["tp"]), EP + ("tp",))
    placed = (
        P(EP, "tp"),
        P(EP, "tp"),
        P(EP, None),
        P(EP, None),
        P(EP, None, "tp"),
        P(EP, None, "tp"),
        P(EP, "tp", None),
        P(None, "tp"),
        P(None, "tp"),
        P(None, "tp"),
    )
    return jax.shard_map(
        per_device,
        mesh=split,
        in_specs=placed,
        out_specs=(
            P(EP, "tp"),
            P(EP, None),
            P(EP, None, "tp"),
            P(EP, None, "tp"),
            P(EP, "tp", None),
            P(EP, "tp"),
            P(EP, "tp"),
            P(EP, "tp"),
        ),
        check_vma=False,
    )
```

```python
import jax
import jax.numpy as jnp
from jax import lax
from jax.experimental import pallas as pl
from jax.experimental.pallas import tpu as pltpu
from jax.sharding import Mesh
from jax.sharding import PartitionSpec as P

EP = ("ep_0", "ep_1", "ep_2")
BF = jnp.bfloat16
F32 = jnp.float32
CAP = 3
LANES = 128


def dot(left, right, dims):
    return lax.dot_general(left, right, ((dims[:1], dims[1:]), ((), ())), preferred_element_type=F32)


def silu_parts(preact):
    sigmoid_v = jax.nn.sigmoid(preact)
    return (preact * sigmoid_v, sigmoid_v * (1.0 + preact * (1.0 - sigmoid_v)))


def fused_kernel(
    nz, ny, nx,
    tokens, cotangent, routes_in, weights_in, gate_proj, up_proj, down_proj,
    shared_gate, shared_up, shared_down,
    token_grad, weight_grad, gate_grad, up_grad, down_grad, sgate_grad, sup_grad, sdown_grad,
    wtok, wcot, wgu, wd, sgu, sd,
    routes, route_weights, onehot, wide, wide2, send1, recv1, fwd1, rows, cots,
    pre, back, hidden, delta, part, part_in, prod, prod_in, prod_out, prod_home,
    send2, recv2, home, mix, mix_in, mix_sum, smix, shid,
    ga, gb, ra1, rb1, sa2, sb2, ra2, rb2, sa3, sb3, ra3, rb3,
    load_sem, tp_send, tp_recv, s1_sem, r1_sem, f_send, f_recv, p_send, p_recv,
    m_send, m_recv, s2_sem, r2_sem, q_send, q_recv, rs_send, rs_recv,
):
    z, y, x, c = (lax.axis_index(n) for n in EP + ("tp",))
    chips = nz * ny * nx
    plane = ny * nx
    me = (z * ny + y) * nx + x
    toks, half = tokens.shape
    width = 2 * half
    hid = wd.shape[0]
    chunks = half // LANES
    q1 = 2 * CAP * chunks
    q2 = CAP * chunks
    first = pl.ds(pl.multiple_of(c * half, LANES), half)
    second = pl.ds(pl.multiple_of((1 - c) * half, LANES), half)
    partner = (z, y, x, 1 - c)

    def remote(src, dst, send_sem, recv_sem, device):
        return pltpu.make_async_remote_copy(
            src_ref=src, dst_ref=dst, send_sem=send_sem, recv_sem=recv_sem,
            device_id=device, device_id_type=pl.DeviceIdType.MESH,
        )

    def await_bytes(ref, sem):
        pltpu.make_async_copy(ref, ref, sem).wait()

    across = [
        (py, px)
        for py in [lax.rem(y + d, ny) for d in range(ny)]
        for px in [lax.rem(x + d, nx) for d in range(nx)]
    ]

    def for_plane(pz, dz, act):
        for i, (py, px) in enumerate(across):
            if i == 0:
                pl.when(dz != 0)(lambda: act((pz, y, x, c), y * nx + x))
            else:
                act((pz, py, px, c), py * nx + px)

    barrier = pltpu.get_barrier_semaphore()

    def greet(dz, carry):
        def act(device, place):
            pl.semaphore_signal(
                barrier, inc=1, device_id=device, device_id_type=pl.DeviceIdType.MESH
            )

        for_plane(lax.rem(z + dz, nz), dz, act)
        return carry

    lax.fori_loop(0, nz, greet, 0)
    pl.semaphore_signal(barrier, inc=1, device_id=partner, device_id_type=pl.DeviceIdType.MESH)

    loads = [
        pltpu.make_async_copy(src, dst, load_sem.at[i])
        for i, (src, dst) in enumerate(
            (
                (tokens, wtok.at[:, :half]),
                (cotangent, wcot.at[:, :half]),
                (shared_gate.at[first], sgu.at[:half, :hid]),
                (shared_gate.at[second], sgu.at[half:, :hid]),
                (shared_up.at[first], sgu.at[:half, hid:]),
                (shared_up.at[second], sgu.at[half:, hid:]),
                (shared_down.at[first], sd.at[:half]),
                (shared_down.at[second], sd.at[half:]),
                (gate_proj.at[first], wgu.at[:half, :hid]),
                (gate_proj.at[second], wgu.at[half:, :hid]),
                (up_proj.at[first], wgu.at[:half, hid:]),
                (up_proj.at[second], wgu.at[half:, hid:]),
                (down_proj.at[:, first], wd.at[:, :half]),
                (down_proj.at[:, second], wd.at[:, half:]),
                (routes_in, routes),
                (weights_in, route_weights),
            )
        )
    ]
    for copy in loads[14:] + loads[:14]:
        copy.start()

    loads[14].wait()
    loads[15].wait()
    lane = lax.broadcasted_iota(jnp.int32, (chips, toks), 1)
    sub = lax.broadcasted_iota(jnp.int32, (chips, toks), 0)
    picks = [routes[k : k + 1, :] == sub for k in range(2)]
    named = picks[0].astype(F32) + picks[1].astype(F32)
    earlier = dot(named.astype(BF), (sub < lane).astype(BF), (1, 0))
    weight_of = jnp.where(picks[0], route_weights[0:1, :], 0.0) + jnp.where(
        picks[1], route_weights[1:2, :], 0.0
    )
    columns = []
    for r in range(CAP):
        held = jnp.where(earlier == float(r), named, 0.0)
        onehot[r * chips : (r + 1) * chips, :] = held.astype(BF)
        columns.append(jnp.sum(held * weight_of, axis=1, keepdims=True))

    loads[0].wait()
    loads[1].wait()
    for r in range(CAP):
        pick = onehot[r * chips : (r + 1) * chips, :]
        for t, source in enumerate((wtok, wcot)):
            chosen = dot(pick, source[:, :half], (1, 0))
            if t == 1:
                chosen = columns[r] * chosen
            for k in range(chunks):
                wide[pl.ds((t * CAP + r) * chunks + k, chips, stride=q1), :] = chosen[
                    :, k * LANES : (k + 1) * LANES
                ]

    def narrow(i, carry):
        block = wide[pl.ds(pl.multiple_of(i * plane * q1, plane * q1), plane * q1), :]
        send1[pl.ds(i * plane, plane)] = block.reshape(plane, q1, LANES).astype(BF)
        return carry

    lax.fori_loop(0, nz, narrow, 0)
    recv1[me] = send1[me]

    pl.semaphore_wait(barrier, chips)

    trade = [
        remote(ref.at[:, :half], ref.at[:, half:], tp_send.at[i], tp_recv.at[i], partner)
        for i, ref in enumerate((wtok, wcot))
    ]
    for copy in trade:
        copy.start()

    jn = nz // 2

    for g in range(2):

        def launch(j, carry):
            dz = 2 * j + g
            pz = lax.rem(z + dz, nz)

            def act(device, place):
                remote(
                    send1.at[pz * plane + place], recv1.at[me], s1_sem, r1_sem.at[dz], device
                ).start()

            for_plane(pz, dz, act)
            return carry

        lax.fori_loop(0, jn, launch, 0)

    for copy in loads[2:8]:
        copy.wait()
    for copy in trade:
        copy.wait()
    smix[...] = dot(wtok[...], sgu[...], (1, 0))
    mix_back = dot(wcot[...], sd[...], (1, 0))
    mix_act, mix_slope = silu_parts(smix[:, :hid])
    mix_up = smix[:, hid:]
    shid[:, 2 * hid :] = (mix_act * mix_up).astype(BF)
    shid[:, :hid] = (mix_back * mix_up * mix_slope).astype(BF)
    shid[:, hid : 2 * hid] = (mix_back * mix_act).astype(BF)

    zrows = width // nz
    zhalf = nz // 2
    cut = ga.shape[-1]

    def shared_terms(i, carry):
        at = pl.ds(pl.multiple_of(i * zrows, LANES), zrows)
        block = lax.rem(i + c * zhalf, nz)
        one = dot(wtok[:, at], shid[:, : 2 * hid], (0, 0)).astype(BF)
        two = dot(wcot[:, at], shid[:, 2 * hid :], (0, 0)).astype(BF)
        ga[block] = one[:, :cut].reshape(ny, nx, zrows // plane, cut)
        gb[block, :, :, :, : 2 * hid - cut] = one[:, cut:].reshape(
            ny, nx, zrows // plane, 2 * hid - cut
        )
        gb[block, :, :, :, 2 * hid - cut :] = two.reshape(ny, nx, zrows // plane, hid)
        return carry

    lax.fori_loop(0, nz, shared_terms, 0)

    mix[...] = dot(shid[:, : 2 * hid], sgu[half:, :], (1, 1)).astype(BF)
    trade_mix = remote(mix, mix_in, m_send, m_recv, partner)
    trade_mix.start()
    for d in range(1, nx):
        px = lax.rem(x + d, nx)
        remote(ga.at[:, :, px], ra1.at[d - 1], rs_send.at[0], rs_recv.at[0], (z, y, px, c)).start()
    for d in range(1, ny):
        py = lax.rem(y + d, ny)
        remote(gb.at[:, py], rb1.at[d - 1], rs_send.at[1], rs_recv.at[1], (z, py, x, c)).start()
    mix_sum[...] = dot(shid[:, : 2 * hid], sgu[:half, :], (1, 1)).astype(BF).astype(F32)

    def reduce_once():
        await_bytes(ra1, rs_recv.at[0])
        await_bytes(rb1, rs_recv.at[1])

        def first_sum(i, carry):
            total = ga[i, :, x].astype(F32)
            other = gb[i, y].astype(F32)
            for d in range(nx - 1):
                total = total + ra1[d, i].astype(F32)
            for d in range(ny - 1):
                other = other + rb1[d, i].astype(F32)
            sa2[i] = total.astype(BF)
            sb2[i] = other.astype(BF)
            return carry

        lax.fori_loop(0, nz, first_sum, 0)
        for d in range(1, ny):
            py = lax.rem(y + d, ny)
            remote(sa2.at[:, py], ra2.at[d - 1], rs_send.at[2], rs_recv.at[2], (z, py, x, c)).start()
        for d in range(1, nx):
            px = lax.rem(x + d, nx)
            remote(sb2.at[:, px], rb2.at[d - 1], rs_send.at[3], rs_recv.at[3], (z, y, px, c)).start()

    count = jn * plane

    def group_step(g, meanwhile):
        def arrive(j, carry):
            dz = 2 * j + g
            zs = lax.rem(z - dz + nz, nz)
            group = pl.ds(zs * plane, plane)
            if g == 0:

                @pl.when(dz == 0)
                def _():
                    await_bytes(recv1.at[pl.ds(0, plane - 1)], r1_sem.at[0])

                @pl.when(dz != 0)
                def _():
                    await_bytes(recv1.at[pl.ds(0, plane)], r1_sem.at[dz])
            else:
                await_bytes(recv1.at[pl.ds(0, plane)], r1_sem.at[dz])

            remote(
                recv1.at[group], fwd1.at[group], f_send, f_recv.at[dz], partner
            ).start()
            wide[pl.ds(pl.multiple_of(j * plane * q1, plane * q1), plane * q1), :] = (
                recv1[group].astype(F32).reshape(plane * q1, LANES)
            )
            return carry

        lax.fori_loop(0, jn, arrive, 0)

        def spread(source, base):
            for t, target in enumerate((rows, cots)):
                for r in range(CAP):
                    for k in range(chunks):
                        target[
                            (g * CAP + r) * count : (g * CAP + r + 1) * count,
                            base + k * LANES : base + (k + 1) * LANES,
                        ] = source[
                            pl.ds((t * CAP + r) * chunks + k, count, stride=q1), :
                        ].astype(BF)

        spread(wide, 0)
        meanwhile()

        def arrive_other(j, carry):
            dz = 2 * j + g
            zs = lax.rem(z - dz + nz, nz)
            group = pl.ds(zs * plane, plane)
            await_bytes(fwd1.at[pl.ds(0, plane)], f_recv.at[dz])
            wide2[pl.ds(pl.multiple_of(j * plane * q1, plane * q1), plane * q1), :] = (
                fwd1[group].astype(F32).reshape(plane * q1, LANES)
            )
            return carry

        lax.fori_loop(0, jn, arrive_other, 0)
        spread(wide2, half)

        if g == 0:
            for copy in loads[8:14]:
                copy.wait()
        mine = pl.ds(g * CAP * count, CAP * count)
        pre[...] = dot(rows[mine, :], wgu[...], (1, 0))
        back[...] = dot(cots[mine, :], wd[...], (1, 1))
        for r in range(CAP):
            here = pl.ds(r * count, count)
            at = pl.ds((g * CAP + r) * count, count)
            gate_act, gate_slope = silu_parts(pre[here, :hid])
            up_pre = pre[here, hid:]
            grad = back[here, :]
            value = gate_act * up_pre
            hidden[at, :] = value.astype(BF)
            delta[at, :hid] = (grad * up_pre * gate_slope).astype(BF)
            delta[at, hid:] = (grad * gate_act).astype(BF)
            total = jnp.sum(value * grad, axis=1, keepdims=True)
            prod[g, here, :] = jnp.broadcast_to(total, (count, LANES)).astype(BF)

        trade_prod = remote(prod.at[g], prod_in.at[g], p_send.at[2 * g], p_recv.at[2 * g], partner)
        trade_prod.start()
        part[g] = dot(delta[mine, :], wgu[half:, :], (1, 1)).astype(BF)
        trade_part = remote(
            part.at[g], part_in.at[g], p_send.at[2 * g + 1], p_recv.at[2 * g + 1], partner
        )
        trade_part.start()
        own = dot(delta[mine, :], wgu[:half, :], (1, 1)).astype(BF)
        trade_prod.wait()
        products = prod[g].astype(F32) + prod_in[g].astype(F32)
        lanes = lax.broadcasted_iota(jnp.int32, (count, LANES), 1)
        packed = jnp.where(
            lanes == 0,
            products[:count],
            jnp.where(lanes == 1, products[count : 2 * count], products[2 * count :]),
        )
        prod_out[g * count : (g + 1) * count, 0, :] = packed.astype(BF).astype(F32)
        trade_part.wait()
        summed = own.astype(F32) + part_in[g].astype(F32)
        for r in range(CAP):
            for k in range(chunks):
                wide[pl.ds(r * chunks + k, count, stride=q2), :] = summed[
                    r * count : (r + 1) * count, k * LANES : (k + 1) * LANES
                ]

        def narrow_back(j, carry):
            block = wide[pl.ds(pl.multiple_of(j * plane * q2, plane * q2), plane * q2), :]
            send2[pl.ds(g * count + j * plane, plane)] = block.reshape(plane, q2, LANES).astype(BF)
            return carry

        lax.fori_loop(0, jn, narrow_back, 0)
        if g == 0:
            recv2[me] = send2[y * nx + x]
            prod_home[me] = prod_out[y * nx + x]

    def give_back(g):
        def leave(j, carry):
            dz = 2 * j + g
            pz = lax.rem(z - dz + nz, nz)

            def act(device, place):
                index = g * count + j * plane + place
                remote(send2.at[index], recv2.at[me], s2_sem, r2_sem, device).start()
                remote(prod_out.at[index], prod_home.at[me], q_send, q_recv, device).start()

            for_plane(pz, dz, act)
            return carry

        lax.fori_loop(0, jn, leave, 0)

    group_step(0, lambda: None)
    give_back(0)
    trade_mix.wait()
    mix_sum[...] = mix_sum[...] + mix_in[...].astype(F32)
    group_step(1, reduce_once)
    give_back(1)
    await_bytes(ra2, rs_recv.at[2])
    await_bytes(rb2, rs_recv.at[3])

    def second_sum(i, carry):
        total = sa2[i, y].astype(F32)
        other = sb2[i, x].astype(F32)
        for d in range(ny - 1):
            total = total + ra2[d, i].astype(F32)
        for d in range(nx - 1):
            other = other + rb2[d, i].astype(F32)
        sa3[i] = total.astype(BF)
        sb3[i] = other.astype(BF)
        return carry

    lax.fori_loop(0, nz, second_sum, 0)
    for d in range(1, nz):
        pz = lax.rem(z + d, nz)
        remote(sa3.at[pz], ra3.at[d - 1], rs_send.at[4], rs_recv.at[4], (pz, y, x, c)).start()
        remote(sb3.at[pz], rb3.at[d - 1], rs_send.at[5], rs_recv.at[5], (pz, y, x, c)).start()
    def expert_terms(i, carry):
        at = pl.ds(pl.multiple_of(i * zrows, LANES), zrows)
        both = dot(rows[:, at], delta[...], (0, 0)).astype(BF)
        gate_grad[at, :] = both[:, :hid]
        up_grad[at, :] = both[:, hid:]
        down_grad[:, at] = dot(hidden[...], cots[:, at], (0, 0)).astype(BF)
        return carry

    lax.fori_loop(0, nz, expert_terms, 0)
    await_bytes(prod_home.at[pl.ds(0, chips - 1)], q_recv)
    held = onehot[...]
    seen = prod_home[:, 0, :]
    for k in range(2):
        mine = jnp.zeros((chips, toks), F32)
        for r in range(CAP):
            chosen = jnp.where(picks[k], held[r * chips : (r + 1) * chips].astype(F32), 0.0)
            mine = mine + chosen * seen[:, r : r + 1]
        weight_grad[k : k + 1, :] = (
            jnp.sum(mine, axis=0, keepdims=True) / route_weights[k : k + 1, :]
        )
    await_bytes(recv2.at[pl.ds(0, chips - 1)], r2_sem)
    wide[pl.ds(0, chips * q2), :] = recv2[...].astype(F32).reshape(chips * q2, LANES)
    for r in range(CAP):
        for k in range(chunks):
            home[r * chips : (r + 1) * chips, k * LANES : (k + 1) * LANES] = wide[
                pl.ds(r * chunks + k, chips, stride=q2), :
            ].astype(BF)
    token_grad[...] = (mix_sum[...] + dot(held, home[...], (0, 0))).astype(BF)

    await_bytes(ra3, rs_recv.at[4])
    await_bytes(rb3, rs_recv.at[5])
    total = sa3[z].astype(F32)
    other = sb3[z].astype(F32)
    for d in range(nz - 1):
        total = total + ra3[d].astype(F32)
        other = other + rb3[d].astype(F32)
    sgate_grad[...] = total[:, :hid]
    sup_grad[:, : cut - hid] = total[:, hid:]
    sup_grad[:, cut - hid :] = other[:, : 2 * hid - cut]
    sdown_grad[...] = other[:, 2 * hid - cut :]

    await_bytes(send1.at[pl.ds(0, chips - 1)], s1_sem)
    await_bytes(fwd1, f_send)
    await_bytes(send2.at[pl.ds(0, chips - 1)], s2_sem)
    await_bytes(prod_out.at[pl.ds(0, chips - 1)], q_send)
    for i, ref in enumerate((ra1, rb1, ra2, rb2, ra3, rb3)):
        await_bytes(ref, rs_send.at[i])


def store_kernel(*refs):
    sources, targets, sem = refs[:8], refs[8:16], refs[16]
    half = sources[0].shape[1]
    c = lax.axis_index("tp")
    first = pl.ds(pl.multiple_of(c * half, LANES), half)
    second = pl.ds(pl.multiple_of((1 - c) * half, LANES), half)
    pairs = [
        (sources[2].at[:half], targets[2].at[first]),
        (sources[2].at[half:], targets[2].at[second]),
        (sources[3].at[:half], targets[3].at[first]),
        (sources[3].at[half:], targets[3].at[second]),
        (sources[4].at[:, :half], targets[4].at[:, first]),
        (sources[4].at[:, half:], targets[4].at[:, second]),
    ] + [(sources[i], targets[i]) for i in (0, 1, 5, 6, 7)]
    copies = [
        pltpu.make_async_copy(src, dst, sem.at[i]) for i, (src, dst) in enumerate(pairs)
    ]
    for copy in copies:
        copy.start()
    for copy in copies:
        copy.wait()


def per_device(
    tokens, cotangent, routes, route_weights, gate_proj, up_proj, down_proj,
    shared_gate, shared_up, shared_down,
):
    nz, ny, nx = (lax.axis_size(n) for n in EP)
    chips = nz * ny * nx
    toks, half = tokens.shape
    width = 2 * half
    hid = gate_proj.shape[2]
    slots = CAP * chips
    q1, q2 = 2 * CAP * half // LANES, CAP * half // LANES
    rblk = width // chips
    cut = 3 * hid // 2
    hbm = pl.BlockSpec(memory_space=pltpu.HBM)
    vmem = pl.BlockSpec(memory_space=pltpu.VMEM)
    dma = pltpu.SemaphoreType.DMA

    finals = [
        ((toks, half), BF),
        ((2, toks), F32),
        ((width, hid), BF),
        ((width, hid), BF),
        ((hid, width), BF),
        ((rblk, hid), F32),
        ((rblk, hid), F32),
        ((rblk, hid), F32),
    ]

    def kernel(*refs):
        fused_kernel(nz, ny, nx, *refs)

    pin = lambda a: pltpu.with_memory_space_constraint(a, pltpu.HBM)
    outs = pl.pallas_call(
        kernel,
        out_shape=[jax.ShapeDtypeStruct(shape, dtype) for shape, dtype in finals],
        in_specs=[hbm] * 10,
        out_specs=[vmem] * 8,
        scratch_shapes=[
            pltpu.VMEM((toks, width), BF),
            pltpu.VMEM((toks, width), BF),
            pltpu.VMEM((width, 2 * hid), BF),
            pltpu.VMEM((hid, width), BF),
            pltpu.VMEM((width, 2 * hid), BF),
            pltpu.VMEM((width, hid), BF),
            pltpu.VMEM((2, toks), jnp.int32),
            pltpu.VMEM((2, toks), F32),
            pltpu.VMEM((slots, toks), BF),
            pltpu.VMEM((chips * q1, LANES), F32),
            pltpu.VMEM((chips * q1 // 2, LANES), F32),
            pltpu.VMEM((chips, q1, LANES), BF),
            pltpu.VMEM((chips, q1, LANES), BF),
            pltpu.VMEM((chips, q1, LANES), BF),
            pltpu.VMEM((slots, width), BF),
            pltpu.VMEM((slots, width), BF),
            pltpu.VMEM((slots // 2, 2 * hid), F32),
            pltpu.VMEM((slots // 2, hid), F32),
            pltpu.VMEM((slots, hid), BF),
            pltpu.VMEM((slots, 2 * hid), BF),
            pltpu.VMEM((2, slots // 2, half), BF),
            pltpu.VMEM((2, slots // 2, half), BF),
            pltpu.VMEM((2, slots // 2, LANES), BF),
            pltpu.VMEM((2, slots // 2, LANES), BF),
            pltpu.VMEM((chips, 1, LANES), F32),
            pltpu.VMEM((chips, 1, LANES), F32),
            pltpu.VMEM((chips, q2, LANES), BF),
            pltpu.VMEM((chips, q2, LANES), BF),
            pltpu.VMEM((slots, half), BF),
            pltpu.VMEM((toks, half), BF),
            pltpu.VMEM((toks, half), BF),
            pltpu.VMEM((toks, half), F32),
            pltpu.VMEM((toks, 2 * hid), F32),
            pltpu.VMEM((toks, 3 * hid), BF),
            pltpu.VMEM((nz, ny, nx, rblk, cut), BF),
            pltpu.VMEM((nz, ny, nx, rblk, cut), BF),
            pltpu.VMEM((nx - 1, nz, ny, rblk, cut), BF),
            pltpu.VMEM((ny - 1, nz, nx, rblk, cut), BF),
            pltpu.VMEM((nz, ny, rblk, cut), BF),
            pltpu.VMEM((nz, nx, rblk, cut), BF),
            pltpu.VMEM((ny - 1, nz, rblk, cut), BF),
            pltpu.VMEM((nx - 1, nz, rblk, cut), BF),
            pltpu.VMEM((nz, rblk, cut), BF),
            pltpu.VMEM((nz, rblk, cut), BF),
            pltpu.VMEM((nz - 1, rblk, cut), BF),
            pltpu.VMEM((nz - 1, rblk, cut), BF),
            dma((16,)),
            dma((2,)),
            dma((2,)),
            dma,
            dma((nz,)),
            dma,
            dma((nz,)),
            dma((4,)),
            dma((4,)),
            dma,
            dma,
            dma,
            dma,
            dma,
            dma,
            dma((6,)),
            dma((6,)),
        ],
        compiler_params=pltpu.CompilerParams(
            collective_id=0, has_side_effects=True, vmem_limit_bytes=48 << 20
        ),
        name="fused",
    )(
        *map(pin, (tokens, cotangent, routes.T, route_weights.T,
        gate_proj[0], up_proj[0], down_proj[0], shared_gate, shared_up, shared_down))
    )
    outs = pl.pallas_call(
        store_kernel,
        out_shape=[jax.ShapeDtypeStruct(shape, dtype) for shape, dtype in finals],
        in_specs=[vmem] * 8,
        out_specs=[hbm] * 8,
        scratch_shapes=[dma((11,))],
        compiler_params=pltpu.CompilerParams(vmem_limit_bytes=1 << 20),
        name="store",
    )(*outs)
    outs = list(outs)
    outs[1] = outs[1].T
    for i in (2, 3, 4):
        outs[i] = outs[i][None]
    return tuple(outs)


def solution(mesh):
    split = Mesh(mesh.devices.reshape(8, 4, 4, mesh.shape["tp"]), EP + ("tp",))
    placed = (
        P(EP, "tp"),
        P(EP, "tp"),
        P(EP, None),
        P(EP, None),
        P(EP, None, "tp"),
        P(EP, None, "tp"),
        P(EP, "tp", None),
        P(None, "tp"),
        P(None, "tp"),
        P(None, "tp"),
    )
    return jax.shard_map(
        per_device,
        mesh=split,
        in_specs=placed,
        out_specs=(
            P(EP, "tp"),
            P(EP, None),
            P(EP, None, "tp"),
            P(EP, None, "tp"),
            P(EP, "tp", None),
            P(EP, "tp"),
            P(EP, "tp"),
            P(EP, "tp"),
        ),
        check_vma=False,
    )
```

```python
import jax
import jax.numpy as jnp
from jax import lax
from jax.experimental import pallas as pl
from jax.experimental.pallas import tpu as pltpu
from jax.sharding import Mesh
from jax.sharding import PartitionSpec as P

EP = ("ep_0", "ep_1", "ep_2")
BF = jnp.bfloat16
F32 = jnp.float32
CAP = 3
LANES = 128


def dot(left, right, dims):
    return lax.dot_general(left, right, ((dims[:1], dims[1:]), ((), ())), preferred_element_type=F32)


def silu_parts(preact):
    sigmoid_v = jax.nn.sigmoid(preact)
    return (preact * sigmoid_v, sigmoid_v * (1.0 + preact * (1.0 - sigmoid_v)))


def fused_kernel(
    nz, ny, nx,
    tokens, cotangent, routes_in, weights_in, gate_proj, up_proj, down_proj,
    shared_gate, shared_up, shared_down,
    token_grad, weight_grad, gate_grad, up_grad, down_grad, sgate_grad, sup_grad, sdown_grad,
    wtok, wcot, wgu, wd, sgu, sd,
    routes, route_weights, onehot, wide, wide2, send1, recv1, fwd1, rows, cots,
    pre, back, hidden, delta, part, part_in, prod, prod_in, prod_out, prod_home,
    send2, recv2, home, mix, mix_in, mix_sum, smix, shid,
    ga, gb, ra1, rb1, sa2, sb2, ra2, rb2, sa3, sb3, ra3, rb3,
    load_sem, tp_send, tp_recv, s1_sem, r1_sem, f_send, f_recv, p_send, p_recv,
    m_send, m_recv, s2_sem, r2_sem, q_send, q_recv, rs_send, rs_recv,
):
    z, y, x, c = (lax.axis_index(n) for n in EP + ("tp",))
    chips = nz * ny * nx
    plane = ny * nx
    me = (z * ny + y) * nx + x
    toks, half = tokens.shape
    width = 2 * half
    hid = wd.shape[0]
    chunks = half // LANES
    q1 = 2 * CAP * chunks
    q2 = CAP * chunks
    first = pl.ds(pl.multiple_of(c * half, LANES), half)
    second = pl.ds(pl.multiple_of((1 - c) * half, LANES), half)
    partner = (z, y, x, 1 - c)

    def remote(src, dst, send_sem, recv_sem, device):
        return pltpu.make_async_remote_copy(
            src_ref=src, dst_ref=dst, send_sem=send_sem, recv_sem=recv_sem,
            device_id=device, device_id_type=pl.DeviceIdType.MESH,
        )

    def await_bytes(ref, sem):
        pltpu.make_async_copy(ref, ref, sem).wait()

    across = [
        (py, px)
        for py in [lax.rem(y + d, ny) for d in range(ny)]
        for px in [lax.rem(x + d, nx) for d in range(nx)]
    ]

    def for_plane(pz, dz, act):
        for i, (py, px) in enumerate(across):
            if i == 0:
                pl.when(dz != 0)(lambda: act((pz, y, x, c), y * nx + x))
            else:
                act((pz, py, px, c), py * nx + px)

    barrier = pltpu.get_barrier_semaphore()

    def greet(i, carry):
        dz = lax.rem(i + nz // 2, nz)

        def act(device, place):
            pl.semaphore_signal(
                barrier, inc=1, device_id=device, device_id_type=pl.DeviceIdType.MESH
            )

        for_plane(lax.rem(z + dz, nz), dz, act)
        return carry

    lax.fori_loop(0, nz, greet, 0)
    pl.semaphore_signal(barrier, inc=1, device_id=partner, device_id_type=pl.DeviceIdType.MESH)

    loads = [
        pltpu.make_async_copy(src, dst, load_sem.at[i])
        for i, (src, dst) in enumerate(
            (
                (tokens, wtok.at[:, :half]),
                (cotangent, wcot.at[:, :half]),
                (shared_gate.at[first], sgu.at[:half, :hid]),
                (shared_gate.at[second], sgu.at[half:, :hid]),
                (shared_up.at[first], sgu.at[:half, hid:]),
                (shared_up.at[second], sgu.at[half:, hid:]),
                (shared_down.at[first], sd.at[:half]),
                (shared_down.at[second], sd.at[half:]),
                (gate_proj.at[first], wgu.at[:half, :hid]),
                (gate_proj.at[second], wgu.at[half:, :hid]),
                (up_proj.at[first], wgu.at[:half, hid:]),
                (up_proj.at[second], wgu.at[half:, hid:]),
                (down_proj.at[:, first], wd.at[:, :half]),
                (down_proj.at[:, second], wd.at[:, half:]),
                (routes_in, routes),
                (weights_in, route_weights),
            )
        )
    ]
    for copy in loads[14:] + loads[:14]:
        copy.start()

    loads[14].wait()
    loads[15].wait()
    lane = lax.broadcasted_iota(jnp.int32, (chips, toks), 1)
    sub = lax.broadcasted_iota(jnp.int32, (chips, toks), 0)
    picks = [routes[k : k + 1, :] == sub for k in range(2)]
    named = picks[0].astype(F32) + picks[1].astype(F32)
    earlier = dot(named.astype(BF), (sub < lane).astype(BF), (1, 0))
    weight_of = jnp.where(picks[0], route_weights[0:1, :], 0.0) + jnp.where(
        picks[1], route_weights[1:2, :], 0.0
    )
    columns = []
    for r in range(CAP):
        held = jnp.where(earlier == float(r), named, 0.0)
        onehot[r * chips : (r + 1) * chips, :] = held.astype(BF)
        columns.append(jnp.sum(held * weight_of, axis=1, keepdims=True))

    loads[0].wait()
    loads[1].wait()
    for r in range(CAP):
        pick = onehot[r * chips : (r + 1) * chips, :]
        for t, source in enumerate((wtok, wcot)):
            chosen = dot(pick, source[:, :half], (1, 0))
            if t == 1:
                chosen = columns[r] * chosen
            for k in range(chunks):
                wide[pl.ds((t * CAP + r) * chunks + k, chips, stride=q1), :] = chosen[
                    :, k * LANES : (k + 1) * LANES
                ]

    def narrow(i, carry):
        block = wide[pl.ds(pl.multiple_of(i * plane * q1, plane * q1), plane * q1), :]
        send1[pl.ds(i * plane, plane)] = block.reshape(plane, q1, LANES).astype(BF)
        return carry

    lax.fori_loop(0, nz, narrow, 0)
    recv1[me] = send1[me]

    pl.semaphore_wait(barrier, chips)

    trade = [
        remote(ref.at[:, :half], ref.at[:, half:], tp_send.at[i], tp_recv.at[i], partner)
        for i, ref in enumerate((wtok, wcot))
    ]
    for copy in trade:
        copy.start()

    jn = nz // 2
    turn = nz // 2 - 2
    home_j = (nz - turn) % nz // 2

    def plane_step(j, g):
        return lax.rem(2 * j + g + turn, nz)


    def send_rows(g):
        def launch(j, carry):
            dz = plane_step(j, g)
            pz = lax.rem(z + dz, nz)

            def act(device, place):
                remote(
                    send1.at[pz * plane + place], recv1.at[me], s1_sem, r1_sem.at[dz], device
                ).start()

            for_plane(pz, dz, act)
            return carry

        lax.fori_loop(0, jn, launch, 0)

    send_rows(0)

    for copy in loads[2:8]:
        copy.wait()
    for copy in trade:
        copy.wait()
    smix[...] = dot(wtok[...], sgu[...], (1, 0))
    mix_back = dot(wcot[...], sd[...], (1, 0))
    mix_act, mix_slope = silu_parts(smix[:, :hid])
    mix_up = smix[:, hid:]
    shid[:, 2 * hid :] = (mix_act * mix_up).astype(BF)
    shid[:, :hid] = (mix_back * mix_up * mix_slope).astype(BF)
    shid[:, hid : 2 * hid] = (mix_back * mix_act).astype(BF)

    zrows = width // nz
    zhalf = nz // 2
    cut = ga.shape[-1]

    def shared_terms(i, carry):
        at = pl.ds(pl.multiple_of(i * zrows, LANES), zrows)
        block = lax.rem(i + c * zhalf, nz)
        one = dot(wtok[:, at], shid[:, : 2 * hid], (0, 0)).astype(BF)
        two = dot(wcot[:, at], shid[:, 2 * hid :], (0, 0)).astype(BF)
        ga[block] = one[:, :cut].reshape(ny, nx, zrows // plane, cut)
        gb[block, :, :, :, : 2 * hid - cut] = one[:, cut:].reshape(
            ny, nx, zrows // plane, 2 * hid - cut
        )
        gb[block, :, :, :, 2 * hid - cut :] = two.reshape(ny, nx, zrows // plane, hid)
        return carry

    lax.fori_loop(0, nz, shared_terms, 0)

    mix[...] = dot(shid[:, : 2 * hid], sgu[half:, :], (1, 1)).astype(BF)
    trade_mix = remote(mix, mix_in, m_send, m_recv, partner)
    trade_mix.start()
    for d in range(1, nx):
        px = lax.rem(x + d, nx)
        remote(ga.at[:, :, px], ra1.at[d - 1], rs_send.at[0], rs_recv.at[0], (z, y, px, c)).start()
    for d in range(1, ny):
        py = lax.rem(y + d, ny)
        remote(gb.at[:, py], rb1.at[d - 1], rs_send.at[1], rs_recv.at[1], (z, py, x, c)).start()
    send_rows(1)
    mix_sum[...] = dot(shid[:, : 2 * hid], sgu[:half, :], (1, 1)).astype(BF).astype(F32)

    def reduce_once():
        await_bytes(ra1, rs_recv.at[0])
        await_bytes(rb1, rs_recv.at[1])

        def first_sum(i, carry):
            total = ga[i, :, x].astype(F32)
            other = gb[i, y].astype(F32)
            for d in range(nx - 1):
                total = total + ra1[d, i].astype(F32)
            for d in range(ny - 1):
                other = other + rb1[d, i].astype(F32)
            sa2[i] = total.astype(BF)
            sb2[i] = other.astype(BF)
            return carry

        lax.fori_loop(0, nz, first_sum, 0)
        for d in range(1, ny):
            py = lax.rem(y + d, ny)
            remote(sa2.at[:, py], ra2.at[d - 1], rs_send.at[2], rs_recv.at[2], (z, py, x, c)).start()
        for d in range(1, nx):
            px = lax.rem(x + d, nx)
            remote(sb2.at[:, px], rb2.at[d - 1], rs_send.at[3], rs_recv.at[3], (z, y, px, c)).start()

    count = jn * plane

    def group_step(g):
        def arrive(j, carry):
            dz = plane_step(j, g)
            zs = lax.rem(z - dz + nz, nz)
            group = pl.ds(zs * plane, plane)
            if g == 0:

                @pl.when(dz == 0)
                def _():
                    await_bytes(recv1.at[pl.ds(0, plane - 1)], r1_sem.at[0])

                @pl.when(dz != 0)
                def _():
                    await_bytes(recv1.at[pl.ds(0, plane)], r1_sem.at[dz])
            else:
                await_bytes(recv1.at[pl.ds(0, plane)], r1_sem.at[dz])

            remote(
                recv1.at[group], fwd1.at[group], f_send, f_recv.at[dz], partner
            ).start()
            wide[pl.ds(pl.multiple_of(j * plane * q1, plane * q1), plane * q1), :] = (
                recv1[group].astype(F32).reshape(plane * q1, LANES)
            )
            return carry

        lax.fori_loop(0, jn, arrive, 0)

        def spread(source, base):
            for t, target in enumerate((rows, cots)):
                for r in range(CAP):
                    for k in range(chunks):
                        target[
                            (g * CAP + r) * count : (g * CAP + r + 1) * count,
                            base + k * LANES : base + (k + 1) * LANES,
                        ] = source[
                            pl.ds((t * CAP + r) * chunks + k, count, stride=q1), :
                        ].astype(BF)

        spread(wide, 0)

        def arrive_other(j, carry):
            dz = plane_step(j, g)
            zs = lax.rem(z - dz + nz, nz)
            group = pl.ds(zs * plane, plane)
            await_bytes(fwd1.at[pl.ds(0, plane)], f_recv.at[dz])
            wide2[pl.ds(pl.multiple_of(j * plane * q1, plane * q1), plane * q1), :] = (
                fwd1[group].astype(F32).reshape(plane * q1, LANES)
            )
            return carry

        lax.fori_loop(0, jn, arrive_other, 0)
        spread(wide2, half)

        if g == 0:
            for copy in loads[8:14]:
                copy.wait()
        mine = pl.ds(g * CAP * count, CAP * count)
        pre[...] = dot(rows[mine, :], wgu[...], (1, 0))
        back[...] = dot(cots[mine, :], wd[...], (1, 1))
        for r in range(CAP):
            here = pl.ds(r * count, count)
            at = pl.ds((g * CAP + r) * count, count)
            gate_act, gate_slope = silu_parts(pre[here, :hid])
            up_pre = pre[here, hid:]
            grad = back[here, :]
            value = gate_act * up_pre
            hidden[at, :] = value.astype(BF)
            delta[at, :hid] = (grad * up_pre * gate_slope).astype(BF)
            delta[at, hid:] = (grad * gate_act).astype(BF)
            total = jnp.sum(value * grad, axis=1, keepdims=True)
            prod[g, here, :] = jnp.broadcast_to(total, (count, LANES)).astype(BF)

        trade_prod = remote(prod.at[g], prod_in.at[g], p_send.at[2 * g], p_recv.at[2 * g], partner)
        trade_prod.start()
        part[g] = dot(delta[mine, :], wgu[half:, :], (1, 1)).astype(BF)
        trade_part = remote(
            part.at[g], part_in.at[g], p_send.at[2 * g + 1], p_recv.at[2 * g + 1], partner
        )
        trade_part.start()
        own = dot(delta[mine, :], wgu[:half, :], (1, 1)).astype(BF)
        trade_prod.wait()
        products = prod[g].astype(F32) + prod_in[g].astype(F32)
        lanes = lax.broadcasted_iota(jnp.int32, (count, LANES), 1)
        packed = jnp.where(
            lanes == 0,
            products[:count],
            jnp.where(lanes == 1, products[count : 2 * count], products[2 * count :]),
        )
        prod_out[g * count : (g + 1) * count, 0, :] = packed.astype(BF).astype(F32)
        trade_part.wait()
        summed = own.astype(F32) + part_in[g].astype(F32)
        for r in range(CAP):
            for k in range(chunks):
                wide[pl.ds(r * chunks + k, count, stride=q2), :] = summed[
                    r * count : (r + 1) * count, k * LANES : (k + 1) * LANES
                ]

        def narrow_back(j, carry):
            block = wide[pl.ds(pl.multiple_of(j * plane * q2, plane * q2), plane * q2), :]
            send2[pl.ds(g * count + j * plane, plane)] = block.reshape(plane, q2, LANES).astype(BF)
            return carry

        lax.fori_loop(0, jn, narrow_back, 0)
        if g == 0:
            recv2[me] = send2[home_j * plane + y * nx + x]
            prod_home[me] = prod_out[home_j * plane + y * nx + x]

    def give_back(g):
        def over_planes(act_on):
            def leave(j, carry):
                dz = plane_step(j, g)
                pz = lax.rem(z - dz + nz, nz)

                def act(device, place):
                    act_on(g * count + j * plane + place, device)

                for_plane(pz, dz, act)
                return carry

            lax.fori_loop(0, jn, leave, 0)

        def product(index, device):
            remote(prod_out.at[index], prod_home.at[me], q_send, q_recv, device).start()

        def row(index, device):
            remote(send2.at[index], recv2.at[me], s2_sem, r2_sem.at[g], device).start()

        over_planes(product)
        over_planes(row)

    group_step(0)
    give_back(0)
    trade_mix.wait()
    mix_sum[...] = mix_sum[...] + mix_in[...].astype(F32)
    group_step(1)
    reduce_once()
    give_back(1)
    def expert_terms(i, carry):
        at = pl.ds(pl.multiple_of(i * zrows, LANES), zrows)
        both = dot(rows[:, at], delta[...], (0, 0)).astype(BF)
        gate_grad[at, :] = both[:, :hid]
        up_grad[at, :] = both[:, hid:]
        down_grad[:, at] = dot(hidden[...], cots[:, at], (0, 0)).astype(BF)
        return carry

    lax.fori_loop(0, nz, expert_terms, 0)
    await_bytes(ra2, rs_recv.at[2])
    await_bytes(rb2, rs_recv.at[3])

    def second_sum(i, carry):
        total = sa2[i, y].astype(F32)
        other = sb2[i, x].astype(F32)
        for d in range(ny - 1):
            total = total + ra2[d, i].astype(F32)
        for d in range(nx - 1):
            other = other + rb2[d, i].astype(F32)
        sa3[i] = total.astype(BF)
        sb3[i] = other.astype(BF)
        return carry

    lax.fori_loop(0, nz, second_sum, 0)
    for d in range(1, nz):
        pz = lax.rem(z + d, nz)
        remote(sa3.at[pz], ra3.at[d - 1], rs_send.at[4], rs_recv.at[4], (pz, y, x, c)).start()
        remote(sb3.at[pz], rb3.at[d - 1], rs_send.at[5], rs_recv.at[5], (pz, y, x, c)).start()
    def reopen(g):
        await_bytes(recv2.at[pl.ds(0, count - 1 + g)], r2_sem.at[g])

        def plane_rows(j, carry):
            zs = lax.rem(z + 2 * j + g, nz)
            at = pl.ds(zs * plane, plane)
            wide[pl.ds(pl.multiple_of(zs * plane * q2, plane * q2), plane * q2), :] = (
                recv2[at].astype(F32).reshape(plane * q2, LANES)
            )
            for r in range(CAP):
                for k in range(chunks):
                    home[
                        pl.ds(pl.multiple_of(r * chips + zs * plane, plane), plane),
                        k * LANES : (k + 1) * LANES,
                    ] = wide[pl.ds(zs * plane * q2 + r * chunks + k, plane, stride=q2), :].astype(BF)
            return carry

        lax.fori_loop(0, jn, plane_rows, 0)

    reopen(0)
    await_bytes(prod_home.at[pl.ds(0, chips - 1)], q_recv)
    held = onehot[...]
    seen = prod_home[:, 0, :]
    for k in range(2):
        mine = jnp.zeros((chips, toks), F32)
        for r in range(CAP):
            chosen = jnp.where(picks[k], held[r * chips : (r + 1) * chips].astype(F32), 0.0)
            mine = mine + chosen * seen[:, r : r + 1]
        weight_grad[k : k + 1, :] = (
            jnp.sum(mine, axis=0, keepdims=True) / route_weights[k : k + 1, :]
        )
    reopen(1)
    token_grad[...] = (mix_sum[...] + dot(held, home[...], (0, 0))).astype(BF)

    await_bytes(ra3, rs_recv.at[4])
    await_bytes(rb3, rs_recv.at[5])
    total = sa3[z].astype(F32)
    other = sb3[z].astype(F32)
    for d in range(nz - 1):
        total = total + ra3[d].astype(F32)
        other = other + rb3[d].astype(F32)
    sgate_grad[...] = total[:, :hid]
    sup_grad[:, : cut - hid] = total[:, hid:]
    sup_grad[:, cut - hid :] = other[:, : 2 * hid - cut]
    sdown_grad[...] = other[:, 2 * hid - cut :]

    await_bytes(send1.at[pl.ds(0, chips - 1)], s1_sem)
    await_bytes(fwd1, f_send)
    await_bytes(send2.at[pl.ds(0, chips - 1)], s2_sem)
    await_bytes(prod_out.at[pl.ds(0, chips - 1)], q_send)
    for i, ref in enumerate((ra1, rb1, ra2, rb2, ra3, rb3)):
        await_bytes(ref, rs_send.at[i])


def store_kernel(*refs):
    sources, targets, sem = refs[:8], refs[8:16], refs[16]
    half = sources[0].shape[1]
    c = lax.axis_index("tp")
    first = pl.ds(pl.multiple_of(c * half, LANES), half)
    second = pl.ds(pl.multiple_of((1 - c) * half, LANES), half)
    pairs = [
        (sources[2].at[:half], targets[2].at[first]),
        (sources[2].at[half:], targets[2].at[second]),
        (sources[3].at[:half], targets[3].at[first]),
        (sources[3].at[half:], targets[3].at[second]),
        (sources[4].at[:, :half], targets[4].at[:, first]),
        (sources[4].at[:, half:], targets[4].at[:, second]),
    ] + [(sources[i], targets[i]) for i in (0, 1, 5, 6, 7)]
    copies = [
        pltpu.make_async_copy(src, dst, sem.at[i]) for i, (src, dst) in enumerate(pairs)
    ]
    for copy in copies:
        copy.start()
    for copy in copies:
        copy.wait()


def per_device(
    tokens, cotangent, routes, route_weights, gate_proj, up_proj, down_proj,
    shared_gate, shared_up, shared_down,
):
    nz, ny, nx = (lax.axis_size(n) for n in EP)
    chips = nz * ny * nx
    toks, half = tokens.shape
    width = 2 * half
    hid = gate_proj.shape[2]
    slots = CAP * chips
    q1, q2 = 2 * CAP * half // LANES, CAP * half // LANES
    rblk = width // chips
    cut = 3 * hid // 2
    hbm = pl.BlockSpec(memory_space=pltpu.HBM)
    vmem = pl.BlockSpec(memory_space=pltpu.VMEM)
    dma = pltpu.SemaphoreType.DMA

    finals = [
        ((toks, half), BF),
        ((2, toks), F32),
        ((width, hid), BF),
        ((width, hid), BF),
        ((hid, width), BF),
        ((rblk, hid), F32),
        ((rblk, hid), F32),
        ((rblk, hid), F32),
    ]

    def kernel(*refs):
        fused_kernel(nz, ny, nx, *refs)

    pin = lambda a: pltpu.with_memory_space_constraint(a, pltpu.HBM)
    outs = pl.pallas_call(
        kernel,
        out_shape=[jax.ShapeDtypeStruct(shape, dtype) for shape, dtype in finals],
        in_specs=[hbm] * 10,
        out_specs=[vmem] * 8,
        scratch_shapes=[
            pltpu.VMEM((toks, width), BF),
            pltpu.VMEM((toks, width), BF),
            pltpu.VMEM((width, 2 * hid), BF),
            pltpu.VMEM((hid, width), BF),
            pltpu.VMEM((width, 2 * hid), BF),
            pltpu.VMEM((width, hid), BF),
            pltpu.VMEM((2, toks), jnp.int32),
            pltpu.VMEM((2, toks), F32),
            pltpu.VMEM((slots, toks), BF),
            pltpu.VMEM((chips * q1, LANES), F32),
            pltpu.VMEM((chips * q1 // 2, LANES), F32),
            pltpu.VMEM((chips, q1, LANES), BF),
            pltpu.VMEM((chips, q1, LANES), BF),
            pltpu.VMEM((chips, q1, LANES), BF),
            pltpu.VMEM((slots, width), BF),
            pltpu.VMEM((slots, width), BF),
            pltpu.VMEM((slots // 2, 2 * hid), F32),
            pltpu.VMEM((slots // 2, hid), F32),
            pltpu.VMEM((slots, hid), BF),
            pltpu.VMEM((slots, 2 * hid), BF),
            pltpu.VMEM((2, slots // 2, half), BF),
            pltpu.VMEM((2, slots // 2, half), BF),
            pltpu.VMEM((2, slots // 2, LANES), BF),
            pltpu.VMEM((2, slots // 2, LANES), BF),
            pltpu.VMEM((chips, 1, LANES), F32),
            pltpu.VMEM((chips, 1, LANES), F32),
            pltpu.VMEM((chips, q2, LANES), BF),
            pltpu.VMEM((chips, q2, LANES), BF),
            pltpu.VMEM((slots, half), BF),
            pltpu.VMEM((toks, half), BF),
            pltpu.VMEM((toks, half), BF),
            pltpu.VMEM((toks, half), F32),
            pltpu.VMEM((toks, 2 * hid), F32),
            pltpu.VMEM((toks, 3 * hid), BF),
            pltpu.VMEM((nz, ny, nx, rblk, cut), BF),
            pltpu.VMEM((nz, ny, nx, rblk, cut), BF),
            pltpu.VMEM((nx - 1, nz, ny, rblk, cut), BF),
            pltpu.VMEM((ny - 1, nz, nx, rblk, cut), BF),
            pltpu.VMEM((nz, ny, rblk, cut), BF),
            pltpu.VMEM((nz, nx, rblk, cut), BF),
            pltpu.VMEM((ny - 1, nz, rblk, cut), BF),
            pltpu.VMEM((nx - 1, nz, rblk, cut), BF),
            pltpu.VMEM((nz, rblk, cut), BF),
            pltpu.VMEM((nz, rblk, cut), BF),
            pltpu.VMEM((nz - 1, rblk, cut), BF),
            pltpu.VMEM((nz - 1, rblk, cut), BF),
            dma((16,)),
            dma((2,)),
            dma((2,)),
            dma,
            dma((nz,)),
            dma,
            dma((nz,)),
            dma((4,)),
            dma((4,)),
            dma,
            dma,
            dma,
            dma((2,)),
            dma,
            dma,
            dma((6,)),
            dma((6,)),
        ],
        compiler_params=pltpu.CompilerParams(
            collective_id=0, has_side_effects=True, vmem_limit_bytes=48 << 20
        ),
        name="fused",
    )(
        *map(pin, (tokens, cotangent, routes.T, route_weights.T,
        gate_proj[0], up_proj[0], down_proj[0], shared_gate, shared_up, shared_down))
    )
    outs = pl.pallas_call(
        store_kernel,
        out_shape=[jax.ShapeDtypeStruct(shape, dtype) for shape, dtype in finals],
        in_specs=[vmem] * 8,
        out_specs=[hbm] * 8,
        scratch_shapes=[dma((11,))],
        compiler_params=pltpu.CompilerParams(vmem_limit_bytes=1 << 20),
        name="store",
    )(*outs)
    outs = list(outs)
    outs[1] = outs[1].T
    for i in (2, 3, 4):
        outs[i] = outs[i][None]
    return tuple(outs)


def solution(mesh):
    split = Mesh(mesh.devices.reshape(8, 4, 4, mesh.shape["tp"]), EP + ("tp",))
    placed = (
        P(EP, "tp"),
        P(EP, "tp"),
        P(EP, None),
        P(EP, None),
        P(EP, None, "tp"),
        P(EP, None, "tp"),
        P(EP, "tp", None),
        P(None, "tp"),
        P(None, "tp"),
        P(None, "tp"),
    )
    return jax.shard_map(
        per_device,
        mesh=split,
        in_specs=placed,
        out_specs=(
            P(EP, "tp"),
            P(EP, None),
            P(EP, None, "tp"),
            P(EP, None, "tp"),
            P(EP, "tp", None),
            P(EP, "tp"),
            P(EP, "tp"),
            P(EP, "tp"),
        ),
        check_vma=False,
    )
```
